32 devices in a mesh: grp: 2 (over y), dp: 2 (over x), kv: 4 (over z), tp: 2 (over core).
Axes of the slice: x: 2, y: 2, z: 4, core: 2. Of those that a mesh axis runs over, the one named last changes fastest.
Arguments:
- tokens: bfloat16 [256, 4, 4096], P(('grp', 'dp'), None, ('kv', 'tp')), parts along dimension 0, may hold values from -160 to 160
- norm_gain: float32 [4096], replicated, may hold values from 0.1 to 1.9
- w_query: bfloat16 [4096, 16, 64], P(None, 'kv'), may hold values from -0.09375 to 0.09375
- w_key: bfloat16 [4096, 16, 64], P(None, 'kv'), may hold values from -0.09375 to 0.09375
- w_value: bfloat16 [4096, 16, 128], P(None, 'kv', 'tp'), may hold values from -0.09375 to 0.09375
- w_outgate: bfloat16 [4096, 16, 128], P(None, 'kv', 'tp'), may hold values from -0.09375 to 0.09375
- w_input: bfloat16 [4096, 16], replicated, may hold values from -0.09375 to 0.09375
- w_forget: bfloat16 [4096, 16], replicated, may hold values from -0.09375 to 0.09375
- forget_bias: float32 [16], replicated, may hold values from -1 to 4
- head_gain: float32 [16, 128], replicated, may hold values from 0.1 to 1.9
- w_out: bfloat16 [16, 128, 4096], P('kv', 'tp'), may hold values from -0.125 to 0.125
- memory: float32 [256, 16, 128, 64], P(('grp', 'dp'), 'kv', 'tp'), parts along dimension 0, may hold values from -12 to 12
- normalizer: float32 [256, 16, 64], P(('grp', 'dp'), 'kv'), parts along dimension 0, may hold values from -12 to 12
- stabilizer: float32 [256, 16], P(('grp', 'dp'), 'kv'), parts along dimension 0, may hold values from -1 to 1
- prev_keys: bfloat16 [256, 4, 16, 64], P(('grp', 'dp'), None, 'kv'), parts along dimension 0, may hold values from -6 to 6
- prev_values: bfloat16 [256, 4, 16, 128], P(('grp', 'dp'), None, 'kv', 'tp'), parts along dimension 0, may hold values from -6 to 6
- prev_input: float32 [256, 4, 16], P(('grp', 'dp'), None, 'kv'), parts along dimension 0, may hold values from -4 to 4
- prev_forget: float32 [256, 4, 16], P(('grp', 'dp'), None, 'kv'), parts along dimension 0, may hold values from -2 to -0.02
- accepted: int32 [256], P(('grp', 'dp')), parts along dimension 0, may hold values from 0 to 4
Outputs:
- mixed: bfloat16 [256, 4, 4096], P(('grp', 'dp'), None, ('kv', 'tp')), parts along dimension 0
- new_memory: float32 [256, 16, 128, 64], P(('grp', 'dp'), 'kv', 'tp'), parts along dimension 0
- new_normalizer: float32 [256, 16, 64], P(('grp', 'dp'), 'kv'), parts along dimension 0
- new_stabilizer: float32 [256, 16], P(('grp', 'dp'), 'kv'), parts along dimension 0
- new_keys: bfloat16 [256, 4, 16, 64], P(('grp', 'dp'), None, 'kv'), parts along dimension 0
- new_values: bfloat16 [256, 4, 16, 128], P(('grp', 'dp'), None, 'kv', 'tp'), parts along dimension 0
- new_input: float32 [256, 4, 16], P(('grp', 'dp'), None, 'kv'), parts along dimension 0
- new_forget: float32 [256, 4, 16], P(('grp', 'dp'), None, 'kv'), parts along dimension 0
The draws below stay inside these ranges and needn't reach their ends.
There are 2 independent parts, one for each index of `grp`. The reference program is written for one: setup_inputs(seed, part) draws one part's arguments, and reference() takes and returns one part's arrays. A program takes and returns all parts, laid end to end along the dimension named above; an argument that names none is the same for every part. Nothing has to cross between parts.
All inputs are finite; a program needn't handle non-finite values.
Results may differ from the reference program's by a relative error of at most 0.038.
Values may be sent and summed in bfloat16 or wider, within the bound.
A program may use at most 128 MiB of HBM per device.

```python
import math
import jax
import jax.numpy as jnp
from jax import lax

D = 4096
HEADS = 16
DK = 64
DV = 128
PROPOSALS = 4
SEQS = 128


def draw_tokens(key, part):
    base_key, row_key = jax.random.split(jax.random.fold_in(key, 17))
    position = jnp.arange(D, dtype=jnp.float32) / (D - 1)
    base = jnp.clip(jax.random.normal(base_key, (SEQS, PROPOSALS, D), jnp.float32), -4.0, 4.0)
    column = jnp.exp(math.log(3.0) * position)
    row_scale = jnp.exp(jax.random.uniform(row_key, (SEQS, PROPOSALS, 1), jnp.float32, 0.0, math.log(10.0)))
    return (base * column * row_scale).astype(jnp.bfloat16)


def with_ends(result, stream_key, low, largest):
    extent = result.shape
    place = [jax.random.randint(jax.random.fold_in(stream_key, axis), (), 0, extent[axis]) for axis in range(len(extent))]
    result = result.at[tuple(place)].set(low)
    longest = extent.index(max(extent))
    place[longest] = (place[longest] + 1) % extent[longest]
    return result.at[tuple(place)].set(largest)


def block_scale(own_key, shape, shards, least, high):
    def one(dim, shards_of):
        heights = jax.random.uniform(jax.random.fold_in(jax.random.fold_in(own_key, 6), dim), (shards_of,), jnp.float32, least / len(shards), high / len(shards))
        return jnp.repeat(jnp.exp(heights), shape[dim] // shards_of).reshape((-1,) + (1,) * (len(shape) - dim - 1))

    gain = one(*shards[0])
    for cut in shards[1:]:
        gain = gain * one(*cut)
    return gain


def bell_draw(key, extent, scale, reach, shards=(), kind=jnp.bfloat16):
    values = jax.random.normal(key, extent, jnp.float32) * scale
    if len(shards) > 0:
        values = block_scale(key, extent, shards, -0.22, 0.18) * values
    return jnp.clip(values, min=-reach, max=reach).astype(kind)


def setup_inputs(seed: int = 0, part: int = 0) -> dict:
    key_list = jax.random.split(jax.random.key(seed), 20)
    own_keys = jax.random.split(jax.random.fold_in(key_list[19], part), 20)
    tokens = draw_tokens(jax.random.fold_in(jax.random.fold_in(key_list[19], part), 71), part)
    norm_gain = jnp.clip(1.0 + 0.18 * jax.random.normal(key_list[1], (D,), jnp.float32), 0.1, 1.9)
    w_query = bell_draw(key_list[2], (D, HEADS, DK), D ** -0.5, 0.09375, ((1, 4),))
    w_key = bell_draw(key_list[3], (D, HEADS, DK), D ** -0.5, 0.09375, ((1, 4),))
    w_value = bell_draw(key_list[4], (D, HEADS, DV), D ** -0.5, 0.09375, ((1, 4), (2, 2)))
    w_outgate = bell_draw(key_list[5], (D, HEADS, DV), D ** -0.5, 0.09375, ((1, 4), (2, 2)))
    w_input = bell_draw(key_list[6], (D, HEADS), D ** -0.5, 0.09375)
    w_forget = bell_draw(key_list[7], (D, HEADS), D ** -0.5, 0.09375)
    forget_bias = jnp.clip(jax.random.uniform(key_list[8], (HEADS,), jnp.float32, -1.0, 4.0), -1.0, 4.0)
    head_gain = jnp.clip(1.0 + 0.18 * jax.random.normal(key_list[9], (HEADS, DV), jnp.float32), 0.1, 1.9)
    w_out = bell_draw(key_list[10], (HEADS, DV, D), (HEADS * DV) ** -0.5, 0.125, ((0, 4), (1, 2)))
    memory = bell_draw(own_keys[11], (SEQS, HEADS, DV, DK), 2.0, 12.0, ((0, 2), (1, 4), (2, 2)), jnp.float32)
    normalizer = bell_draw(own_keys[12], (SEQS, HEADS, DK), 2.0, 12.0, ((0, 2), (1, 4)), jnp.float32)
    stabilizer = jnp.clip(jax.random.uniform(own_keys[13], (SEQS, HEADS), jnp.float32, -1.0, 1.0) * block_scale(own_keys[13], (SEQS, HEADS), ((0, 2), (1, 4)), -0.4, 0.0), -1.0, 1.0)
    prev_keys = bell_draw(own_keys[14], (SEQS, PROPOSALS, HEADS, DK), 1.0, 6.0, ((0, 2), (2, 4)))
    prev_values = bell_draw(own_keys[15], (SEQS, PROPOSALS, HEADS, DV), 1.0, 6.0, ((0, 2), (2, 4), (3, 2)))
    prev_input = bell_draw(own_keys[16], (SEQS, PROPOSALS, HEADS), 1.0, 4.0, ((0, 2), (2, 4)), jnp.float32)
    prev_forget = jnp.clip(-2.0 + 1.98 * jax.random.uniform(own_keys[17], (SEQS, PROPOSALS, HEADS), jnp.float32) ** block_scale(own_keys[17], (SEQS, PROPOSALS, HEADS), ((0, 2), (2, 4)), -0.2, 0.2), -2.0, -0.02)
    accepted = with_ends(jax.random.randint(own_keys[18], (SEQS,), 0, PROPOSALS + 1), jax.random.fold_in(own_keys[18], 1), 0, PROPOSALS).astype(jnp.int32)
    return dict(tokens=tokens, norm_gain=norm_gain, w_query=w_query, w_key=w_key, w_value=w_value, w_outgate=w_outgate, w_input=w_input, w_forget=w_forget, forget_bias=forget_bias, head_gain=head_gain, w_out=w_out, memory=memory, normalizer=normalizer, stabilizer=stabilizer, prev_keys=prev_keys, prev_values=prev_values, prev_input=prev_input, prev_forget=prev_forget, accepted=accepted)


EPS = 1e-06
FAR_NEGATIVE = -1e+30
HIGHEST_PRECISION = lax.Precision.HIGHEST

def recurrent(query_f, key_all, value_all, gate_in, gate_forget, accepted, memory, normalizer, stabilizer):
    proposals = query_f.shape[1]
    total_span = key_all.shape[1]
    position = jnp.arange(total_span, dtype=jnp.int32)
    dropped = (position[None, :] < proposals) & (position[None, :] >= accepted[:, None])
    forget = jnp.where(dropped[:, :, None], 0.0, gate_forget)
    inflow = jnp.where(dropped[:, :, None], FAR_NEGATIVE, gate_in)
    running = jnp.cumsum(forget, axis=1)
    latest = running[:, proposals:]
    spread = latest[:, :, None, :] - running[:, None, :, :] + inflow[:, None, :, :]
    causal = position[None, :] <= (proposals + jnp.arange(proposals, dtype=jnp.int32))[:, None]
    spread = jnp.where(causal[None, :, :, None], spread, FAR_NEGATIVE)
    carried = latest + stabilizer[:, None, :]
    ceiling = jnp.maximum(lax.optimization_barrier(jnp.max(spread, axis=2)), carried)
    scores = jnp.einsum('sthk,suhk->stuh', query_f, key_all, precision=HIGHEST_PRECISION)
    weights = jnp.exp(spread - ceiling[:, :, None, :]) * scores
    carry_scale = jnp.exp(carried - ceiling)
    numerator = jnp.einsum('stuh,suhv->sthv', weights, value_all, precision=HIGHEST_PRECISION)
    numerator = numerator + carry_scale[..., None] * jnp.einsum('shvk,sthk->sthv', memory, query_f, precision=HIGHEST_PRECISION)
    denominator = lax.optimization_barrier(jnp.sum(weights, axis=2)) + carry_scale * jnp.einsum('shk,sthk->sth', normalizer, query_f, precision=HIGHEST_PRECISION)
    cell_out = numerator / jnp.maximum(jnp.abs(denominator), jnp.exp(-ceiling))[..., None]
    boundary = running[:, proposals - 1]
    reached = boundary[:, None, :] - running[:, :proposals] + inflow[:, :proposals]
    new_stabilizer = jnp.maximum(boundary + stabilizer, lax.optimization_barrier(jnp.max(reached, axis=1)))
    decay_old = jnp.exp(boundary + stabilizer - new_stabilizer)
    shares = jnp.exp(reached - new_stabilizer[:, None, :])
    new_memory = decay_old[:, :, None, None] * memory + jnp.einsum('sjh,sjhv,sjhk->shvk', shares, value_all[:, :proposals], key_all[:, :proposals], precision=HIGHEST_PRECISION)
    new_normalizer = decay_old[:, :, None] * normalizer + jnp.einsum('sjh,sjhk->shk', shares, key_all[:, :proposals], precision=HIGHEST_PRECISION)
    return (cell_out, new_memory, new_normalizer, new_stabilizer)

def project(normed, weight):
    return jnp.dot(normed, weight.reshape(weight.shape[0], -1), preferred_element_type=jnp.float32)

def reference(tokens, norm_gain, w_query, w_key, w_value, w_outgate, w_input, w_forget, forget_bias, head_gain, w_out, memory, normalizer, stabilizer, prev_keys, prev_values, prev_input, prev_forget, accepted):
    sequences, proposals, model_width = tokens.shape
    heads = w_query.shape[1]
    key_size = w_query.shape[2]
    value_size = w_value.shape[2]
    as_float = tokens.astype(jnp.float32)
    inv_scale = lax.rsqrt(lax.optimization_barrier(jnp.mean(as_float * as_float, axis=-1, keepdims=True)) + EPS)
    normed = (as_float * inv_scale * norm_gain).astype(jnp.bfloat16).reshape(sequences * proposals, model_width)
    queries = project(normed, w_query).astype(jnp.bfloat16).reshape(sequences, proposals, heads, key_size)
    new_keys = project(normed, w_key).astype(jnp.bfloat16).reshape(sequences, proposals, heads, key_size)
    new_values = project(normed, w_value).astype(jnp.bfloat16).reshape(sequences, proposals, heads, value_size)
    out_gate = project(normed, w_outgate).reshape(sequences, proposals, heads, value_size)
    new_input = project(normed, w_input).reshape(sequences, proposals, heads)
    new_forget = jax.nn.log_sigmoid(project(normed, w_forget).reshape(sequences, proposals, heads) + forget_bias)
    query_f = queries.astype(jnp.float32) * key_size ** (-0.5)
    key_all = jnp.concatenate([prev_keys, new_keys], axis=1).astype(jnp.float32)
    value_all = jnp.concatenate([prev_values, new_values], axis=1).astype(jnp.float32)
    gate_in = jnp.concatenate([prev_input, new_input], axis=1)
    gate_forget = jnp.concatenate([prev_forget, new_forget], axis=1)
    cell_out, new_memory, new_normalizer, new_stabilizer = recurrent(query_f, key_all, value_all, gate_in, gate_forget, accepted, memory, normalizer, stabilizer)
    squares = lax.optimization_barrier(jnp.mean(cell_out * cell_out, axis=-1, keepdims=True))
    gated = (jax.nn.sigmoid(out_gate) * cell_out * lax.rsqrt(squares + EPS) * head_gain).astype(jnp.bfloat16)
    mixed = jnp.dot(gated.reshape(sequences * proposals, heads * value_size), w_out.reshape(heads * value_size, model_width), preferred_element_type=jnp.float32)
    mixed = mixed.astype(jnp.bfloat16).reshape(sequences, proposals, model_width)
    return (mixed, new_memory, new_normalizer, new_stabilizer, new_keys, new_values, new_input, new_forget)
```

```python
import functools
import jax
import jax.numpy as jnp
from jax import lax
from jax.sharding import PartitionSpec as P
from jax.experimental import pallas as pl
from jax.experimental.pallas import tpu as pltpu

EPS = 1e-06
FAR_NEGATIVE = -1e30
HIGHEST = lax.Precision.HIGHEST
MESH = pl.DeviceIdType.MESH
F32 = jnp.float32
BF16 = jnp.bfloat16
VMEM_LIMIT = 60 << 20
HALVES = 2
PIECES = 2
BLOCK = 8


def nn(a, b, precision=None):
    return lax.dot_general(
        a, b, (((1,), (0,)), ((), ())), precision=precision, preferred_element_type=F32
    )


def nt(a, b, precision=None):
    return lax.dot_general(
        a, b, (((1,), (1,)), ((), ())), precision=precision, preferred_element_type=F32
    )


def iota(shape, d):
    return lax.broadcasted_iota(jnp.int32, shape, d)


def enter(n, z, c):
    barrier = pltpu.get_barrier_semaphore()
    pl.semaphore_signal(barrier, inc=1, device_id={"tp": 1 - c}, device_id_type=MESH)

    @pl.when(z > 0)
    def _():
        pl.semaphore_signal(barrier, inc=1, device_id={"kv": z - 1}, device_id_type=MESH)

    @pl.when(z < n - 1)
    def _():
        pl.semaphore_signal(barrier, inc=1, device_id={"kv": z + 1}, device_id_type=MESH)

    peers = 1 + (z > 0).astype(jnp.int32) + (z < n - 1).astype(jnp.int32)
    pl.semaphore_wait(barrier, peers)


def fused_kernel(
    n, key_size, full_values,
    x_ref, gain_ref, bias_ref, pk_ref, pv_ref, pi_ref, pf_ref, acc_ref, stab_ref, nrm_ref, hgain_ref,
    wq_hbm, wk_hbm, wv_hbm, wo_hbm, wi_hbm, wf_hbm, mem_hbm, out_hbm,
    y_out, k_out, v_out, vts, kps, dfull, nn_out, ns_out, ni_out, nf_out,
    xg, weights, acc, squares, mem, packed, nrmb, gates, nsrow, g_own, sq_own, g_in, sq_in, both,
    w_ref, from_low, from_high, to_high, to_low, total_ref,
    load_sem, mem_sem, wload_sem, wsend_sem, wrecv_sem,
    send0, recv0, send1, side1, recv1, ex_send, ex_recv, up_send, up_recv, down_send, down_recv,
):
    z = lax.axis_index("kv")
    c = lax.axis_index("tp")
    seqs, span, width = x_ref.shape
    rows = seqs * span
    lanes = rows // HALVES
    piece = lanes // PIECES
    depth = gain_ref.shape[1]
    keys = key_size
    heads, values = pv_ref.shape[2:]
    hk, hv = heads * keys, heads * values
    blocks = seqs // BLOCK
    hp = nsrow.shape[0]
    up, down, side = {"kv": z + 1}, {"kv": z - 1}, {"tp": 1 - c}

    loads, spans, at = [], [], 0
    for i, src in enumerate((wq_hbm, wk_hbm, wv_hbm, wo_hbm, wi_hbm, wf_hbm)):
        size = src.shape[0]
        spans.append(slice(at, at + size))
        loads.append(
            pltpu.make_async_copy(src, weights.at[pl.ds(at, size)], load_sem.at[i])
        )
        at += size

    def mem_load(b):
        part = pl.ds(b * BLOCK, BLOCK)
        return pltpu.make_async_copy(mem_hbm.at[part], mem.at[part], mem_sem.at[b])

    def own_load(d):
        col = pl.multiple_of((2 * d + c) * width, width)
        return pltpu.make_async_copy(
            out_hbm.at[:, pl.ds(col, width)], w_ref.at[d, pl.ds(0, hv)], wload_sem.at[d]
        )

    def out_piece(d):
        col = pl.multiple_of((2 * d + 1 - c) * width, width)
        return pltpu.make_async_remote_copy(
            src_ref=out_hbm.at[:, pl.ds(col, width)], dst_ref=w_ref.at[d, pl.ds(hv, hv)],
            send_sem=wsend_sem.at[d], recv_sem=wrecv_sem.at[d],
            device_id=side, device_id_type=MESH,
        )

    def hop(slot, p, way, target):
        part = pl.ds(p * piece, piece)
        return pltpu.make_async_remote_copy(
            src_ref=xg.at[slot, 0, part], dst_ref=xg.at[slot, 0, part],
            send_sem=send0.at[way, slot, p], recv_sem=recv0.at[slot, p],
            device_id=target, device_id_type=MESH,
        )

    mine = 2 * z + c

    def direct(target):
        return pltpu.make_async_remote_copy(
            src_ref=xg.at[mine, 1], dst_ref=xg.at[mine, 1],
            send_sem=send1.at[target], recv_sem=recv1.at[mine],
            device_id={"kv": target}, device_id_type=MESH,
        )

    def across(slot):
        return pltpu.make_async_remote_copy(
            src_ref=xg.at[slot, 1], dst_ref=xg.at[slot, 1],
            send_sem=side1.at[slot], recv_sem=recv1.at[slot],
            device_id=side, device_id_type=MESH,
        )

    def arrived(slot):
        return pltpu.make_async_remote_copy(
            src_ref=xg.at[slot, 1], dst_ref=xg.at[slot, 1],
            send_sem=side1.at[slot], recv_sem=recv1.at[slot],
            device_id=side, device_id_type=MESH,
        )

    for load in loads:
        load.start()
    flat = x_ref[...].reshape(rows, width)
    for half in range(HALVES):
        xg[mine, half] = flat[half * lanes : (half + 1) * lanes]
    enter(n, z, c)

    for p in range(PIECES):
        @pl.when(z < n - 1)
        def _():
            hop(mine, p, 0, up).start()

        @pl.when(z > 0)
        def _():
            hop(mine, p, 1, down).start()

    for p in range(PIECES):
        hop(mine, p, 2, side).start()
    across(mine).start()

    @pl.when(z == 0)
    def _():
        direct(z + 1).start()

    @pl.when(z == n - 1)
    def _():
        direct(z - 1).start()

    for b in range(blocks):
        mem_load(b).start()
    for d in range(n):
        own_load(d).start()
        out_piece(d).start()

    acc[...] = jnp.zeros_like(acc)
    squares[...] = jnp.zeros_like(squares)

    expand = (iota((seqs, rows), 0) == iota((seqs, rows), 1) // span).astype(F32)
    lane_pos = iota((span, rows), 1) % span == iota((span, rows), 0)
    dropped = iota((span, seqs), 0) >= acc_ref[...]
    stack, decays, tops = [], [], []
    for h in range(heads):
        stab = stab_ref[h : h + 1, :]
        f = jnp.where(dropped, 0.0, pf_ref[:, h, :])
        i = jnp.where(dropped, FAR_NEGATIVE, pi_ref[:, h, :])
        run = []
        for j in range(span):
            run.append(f[j : j + 1] + run[-1] if run else f[0:1])
        e = run[-1]
        u = e - jnp.concatenate(run, axis=0) + i
        ns = jnp.maximum(e + stab, jnp.max(u, axis=0, keepdims=True))
        ns_out[h : h + 1, :] = ns
        tops.append(ns)
        decays.append(jnp.exp(e + stab - ns))
        stack += [jnp.exp(u - ns), jnp.zeros((8 - span, seqs), F32)]
    tops.append(jnp.zeros((hp - heads, seqs), F32))
    wide = nn(jnp.concatenate(stack + tops, axis=0), expand, HIGHEST)
    nsrow[...] = wide[8 * heads :]
    decays = jnp.concatenate(decays + [jnp.zeros((hp - heads, seqs), F32)], axis=0).T
    old_keys = pk_ref[...].astype(F32).reshape(rows, heads, keys)
    old_values = pv_ref[...].astype(F32).reshape(rows, heads, values)
    odd = (iota((rows, keys), 0) // span) % 2
    spread = iota((seqs, rows), 0) == iota((seqs, rows), 1) // span
    for h in range(heads):
        share_row = jnp.sum(
            jnp.where(lane_pos, wide[8 * h : 8 * h + span], 0.0), axis=0, keepdims=True
        )
        old = old_keys[:, h, :].astype(BF16)
        kps[h] = jnp.concatenate(
            [jnp.where(odd == p, old, jnp.zeros_like(old)) for p in range(2)], axis=1
        )
        part = slice(h * values, (h + 1) * values)
        vts[part, :] = (old_values[:, h, :].T * share_row).astype(BF16)
        full = jnp.broadcast_to(decays[:, h : h + 1], (seqs, keys))
        dfull[h] = full
        after = full * nrm_ref[:, h, :] + nn(jnp.where(spread, share_row, 0.0).astype(BF16), old)
        nn_out[:, h, :] = after
        nrmb[h] = after.astype(BF16)

    def remember(b):
        mem_load(b).wait()
        first = b * BLOCK
        start = pl.multiple_of((first * span) // 128 * 128, 128)
        half = pl.ds(start, 128)
        pair = ((iota((values, 128), 1) + start) // span - first) // 2
        for h in range(heads):
            shared = vts[h * values : (h + 1) * values, half]
            zero = jnp.zeros_like(shared)
            left = jnp.concatenate(
                [jnp.where(pair == s, shared, zero) for s in range(BLOCK // 2)], axis=0
            )
            update = nn(left, kps[h, half, :])
            pairs = []
            for s in range(BLOCK // 2):
                old = jnp.concatenate([mem[first + 2 * s, h], mem[first + 2 * s + 1, h]], axis=1)
                decay = jnp.concatenate(
                    [dfull[h, pl.ds(first + 2 * s + p, 1), :] for p in range(2)], axis=1
                )
                pairs.append((decay * old + update[s * values : (s + 1) * values]).astype(BF16))
            for s in range(BLOCK // 4):
                packed[h, b * (BLOCK // 4) + s] = jnp.concatenate(pairs[2 * s : 2 * s + 2], axis=1)

    def process(owner, half):
        cols = pl.ds(pl.multiple_of(owner * 2 * width, 2 * width), 2 * width)
        x = jnp.concatenate([xg[2 * owner, half], xg[2 * owner + 1, half]], axis=1).astype(F32)
        square = x * x
        total = squares[half]
        for i in range(2 * width // 128):
            total = total + square[:, i * 128 : (i + 1) * 128]
        squares[half] = total
        acc[half] += nt(weights[:, cols], (x * gain_ref[:, cols]).astype(BF16))

    def process_first(owner):
        for p in range(PIECES):
            hop(2 * owner + 1 - c, p, 2, side).wait_recv()
        process(owner, 0)

    def process_second(owner):
        arrived(2 * owner + 1 - c).wait_recv()
        process(owner, 1)

    for load in loads:
        load.wait()
    per = -(-(blocks // HALVES) // (n - 1))

    def gather_first(k, carry):
        for p in range(PIECES):
            @pl.when(z - k >= 0)
            def _():
                slot = 2 * (z - k) + c
                hop(slot, p, 0, up).wait_recv()

                @pl.when(z < n - 1)
                def _():
                    hop(slot, p, 0, up).start()

                hop(slot, p, 2, side).start()

            @pl.when(z + k <= n - 1)
            def _():
                slot = 2 * (z + k) + c
                hop(slot, p, 1, down).wait_recv()

                @pl.when(z > 0)
                def _():
                    hop(slot, p, 1, down).start()

                hop(slot, p, 2, side).start()

        @pl.when((k == z) & (z < n - 1))
        def _():
            direct(z + 1).start()

        @pl.when((k == n - 1 - z) & (z > 0))
        def _():
            direct(z - 1).start()

        @pl.when(z - (k - 1) >= 0)
        def _():
            process_first(z - (k - 1))

        @pl.when((k > 1) & (z + k - 1 <= n - 1))
        def _():
            process_first(z + k - 1)

        for j in range(per):
            b = (k - 1) * per + j

            @pl.when(b < blocks // HALVES)
            def _():
                remember(b)

        return carry

    lax.fori_loop(1, n, gather_first, 0)

    def far(j, carry):
        dist = n - 1 - j

        @pl.when(z + dist <= n - 1)
        def _():
            direct(z + dist).start()

        @pl.when(z - dist >= 0)
        def _():
            direct(z - dist).start()

        return carry

    lax.fori_loop(0, n - 2, far, 0)

    @pl.when(z == n - 1)
    def _():
        process_first(z - (n - 1))

    @pl.when(z == 0)
    def _():
        process_first(z + n - 1)

    place = iota((hp, lanes), 1) % span
    local_gain = hgain_ref[:, :values]
    for i in range(1, hgain_ref.shape[1] // values):
        local_gain = jnp.where(c == i, hgain_ref[:, i * values : (i + 1) * values], local_gain)
    gains = local_gain[:heads]
    for i in range(1, hgain_ref.shape[0] // heads):
        gains = jnp.where(z == i, local_gain[i * heads : (i + 1) * heads], gains)
    columns = jnp.concatenate([gains, jnp.zeros((hp - heads, values), F32)], axis=0).T

    def recur(half):
        part_of = pl.ds(half * lanes, lanes)
        summed = nt(jnp.ones((8, 128), F32), squares[half], HIGHEST)
        inv = lax.rsqrt(summed[0:1] / depth + EPS)
        q, k, v, og, gi, gf = [acc[half, part, :] * inv for part in spans]
        q = (q.astype(BF16).astype(F32) * keys ** (-0.5)).astype(BF16)
        k_rows = k.T.astype(BF16)
        v = v.astype(BF16)
        k_out[part_of, :] = k_rows
        v_out[part_of, :] = v.astype(F32).T.astype(BF16)
        all_heads = gf.shape[0]
        diagonal = iota((all_heads, all_heads), 0) == iota((all_heads, all_heads), 1)
        shift = nn(jnp.where(diagonal, bias_ref[...], 0.0), jnp.ones(gf.shape, F32), HIGHEST)
        raw = gf + shift
        gf = jnp.minimum(raw, 0.0) - jnp.log1p(jnp.exp(-jnp.abs(raw)))
        chosen = []
        for total in (gi, gf):
            out = total[:heads]
            for i in range(1, n):
                out = jnp.where(z == i, total[i * heads : (i + 1) * heads], out)
            chosen.append(jnp.concatenate([out, jnp.zeros((hp - heads, lanes), F32)], axis=0))
        inflow, run = chosen
        gates[0, :, part_of] = inflow
        gates[1, :, part_of] = run
        step = 1
        while step < span:
            run = run + jnp.where(place >= step, pltpu.roll(run, step, 1), 0.0)
            step *= 2
        deltas = [inflow]
        for i in range(1, span):
            spread_i = run - pltpu.roll(run, i, 1) + pltpu.roll(inflow, i, 1)
            deltas.append(jnp.where(place >= i, spread_i, FAR_NEGATIVE))
        carried = run + nsrow[:, part_of]
        top = carried
        for d in deltas:
            top = jnp.maximum(top, d)
        scale = jnp.exp(carried - top)
        floor = jnp.exp(-top)
        ws = [jnp.exp(d - top) for d in deltas]
        placed = []
        for u in range(span):
            w = jnp.zeros_like(top)
            for i in range(span):
                w = jnp.where(place - u == i, ws[i], w)
            placed.append(w)
        same = iota((lanes, lanes), 0) // span == iota((lanes, lanes), 1) // span
        owner = iota(q.shape, 0) // keys
        count = lanes // span
        here = iota((count, lanes), 0) == iota((count, lanes), 1) // span
        quarter = (iota((keys, lanes), 1) // span) % 4
        quad = iota((values, lanes), 1) // span // 4
        for h in range(heads):
            part = slice(h * values, (h + 1) * values)
            query = q[h * keys : (h + 1) * keys]
            none = jnp.zeros_like(query)
            four = jnp.concatenate([jnp.where(quarter == p, query, none) for p in range(4)], axis=0)
            table = packed[h, half * (count // 4) : (half + 1) * (count // 4)]
            read = nn(table.reshape(count // 4 * values, 4 * keys), four)
            recalled = read[:values]
            for s in range(1, count // 4):
                recalled = jnp.where(quad == s, read[s * values : (s + 1) * values], recalled)
            only = jnp.where(owner == h, q, jnp.zeros_like(q))
            w = jnp.concatenate([placed[u][h : h + 1] for u in range(span)] * (8 // span), axis=0)
            w = jnp.broadcast_to(w[None], (lanes // 8, 8, lanes)).reshape(lanes, lanes)
            w = jnp.where(same, w * nn(k_rows, only), 0.0)
            nq = nn(nrmb[h, half * count : (half + 1) * count], query)
            nq = jnp.sum(jnp.where(here, nq, 0.0), axis=0, keepdims=True)
            carry = scale[h : h + 1]
            over = nn(v[part], w.astype(BF16)) + carry * recalled
            under = jnp.sum(w, axis=0, keepdims=True) + carry * nq
            cell = over / jnp.maximum(jnp.abs(under), floor[h : h + 1])
            sq_own[half, h : h + 1, :] = jnp.sum(cell * cell, axis=0, keepdims=True)
            g = jax.nn.sigmoid(og[part]) * cell * columns[:, h : h + 1]
            g_own[half, part, :] = g.astype(BF16)

    def swaps(half):
        return [
            pltpu.make_async_remote_copy(
                src_ref=src.at[half], dst_ref=dst.at[half],
                send_sem=ex_send.at[half, i], recv_sem=ex_recv.at[half, i],
                device_id=side, device_id_type=MESH,
            )
            for i, (src, dst) in enumerate(((g_own, g_in), (sq_own, sq_in)))
        ]

    def join(half):
        for swap in swaps(half):
            swap.wait_recv()
        inv = lax.rsqrt((sq_own[half] + sq_in[half]) / full_values + EPS)
        for i, src in enumerate((g_own, g_in)):
            scaled = jnp.concatenate(
                [
                    src[half, h * values : (h + 1) * values, :].astype(F32) * inv[h : h + 1, :]
                    for h in range(heads)
                ],
                axis=0,
            )
            both[half * lanes : (half + 1) * lanes, i * hv : (i + 1) * hv] = scaled.T.astype(BF16)

    def partial(d, r):
        return nn(both[r * piece : (r + 1) * piece], w_ref[d])

    def upward(d, r):
        return pltpu.make_async_remote_copy(
            src_ref=to_high.at[d, r], dst_ref=from_low.at[d, r],
            send_sem=up_send.at[d, r], recv_sem=up_recv.at[d, r],
            device_id=up, device_id_type=MESH,
        )

    def downward(d, r):
        return pltpu.make_async_remote_copy(
            src_ref=to_low.at[d, r], dst_ref=from_high.at[d, r],
            send_sem=down_send.at[d, r], recv_sem=down_recv.at[d, r],
            device_id=down, device_id_type=MESH,
        )

    def send_first(half):
        def body(i, carry):
            for p in range(PIECES):
                r = half * PIECES + p

                @pl.when(z == 0)
                def _():
                    to_high[n - 1 - i, r] = partial(n - 1 - i, r).astype(BF16)
                    upward(n - 1 - i, r).start()

                @pl.when(z == n - 1)
                def _():
                    to_low[i, r] = partial(i, r).astype(BF16)
                    downward(i, r).start()

            return carry

        lax.fori_loop(0, n - 1, body, 0)

    def send_next(half):
        def body(i, carry):
            high = n - 1 - i + z
            low = i - (n - 1 - z)
            for p in range(PIECES):
                r = half * PIECES + p

                @pl.when((z > 0) & (high > z) & (high <= n - 1))
                def _():
                    term = partial(high, r)
                    upward(high, r).wait_recv()
                    to_high[high, r] = (term + from_low[high, r].astype(F32)).astype(BF16)
                    upward(high, r).start()

                @pl.when((z < n - 1) & (low < z) & (low >= 0))
                def _():
                    term = partial(low, r)
                    downward(low, r).wait_recv()
                    to_low[low, r] = (term + from_high[low, r].astype(F32)).astype(BF16)
                    downward(low, r).start()

            return carry

        lax.fori_loop(0, 2 * n - 2, body, 0)

    recur(0)
    for swap in swaps(0):
        swap.start()

    def rest(b, carry):
        remember(b)
        return carry

    lax.fori_loop(blocks // HALVES, blocks, rest, 0)
    for d in range(n):
        own_load(d).wait()
        out_piece(d).wait_recv()
    join(0)
    send_first(0)

    def gather_second(k, carry):
        @pl.when(z - k >= 0)
        def _():
            slot = 2 * (z - k) + c
            arrived(slot).wait_recv()
            across(slot).start()

        @pl.when(z + k <= n - 1)
        def _():
            slot = 2 * (z + k) + c
            arrived(slot).wait_recv()
            across(slot).start()

        @pl.when(z - (k - 1) >= 0)
        def _():
            process_second(z - (k - 1))

        @pl.when((k > 1) & (z + k - 1 <= n - 1))
        def _():
            process_second(z + k - 1)

        return carry

    lax.fori_loop(1, n, gather_second, 0)

    @pl.when(z == n - 1)
    def _():
        process_second(z - (n - 1))

    @pl.when(z == 0)
    def _():
        process_second(z + n - 1)

    recur(1)
    for swap in swaps(1):
        swap.start()
    join(1)
    send_first(1)
    send_next(0)
    send_next(1)

    for r in range(HALVES * PIECES):
        total_ref[r] = partial(z, r)
    single = [
        jnp.where(lane_pos, gates[i, h : h + 1, :], 0.0) for h in range(heads) for i in range(2)
    ]
    compact = nt(jnp.concatenate(single, axis=0), expand, HIGHEST)
    for h in range(heads):
        ni_out[:, h, :] = compact[2 * h * span : (2 * h + 1) * span]
        nf_out[:, h, :] = compact[(2 * h + 1) * span : (2 * h + 2) * span]
    for r in range(HALVES * PIECES):
        @pl.when(z > 0)
        def _():
            upward(z, r).wait_recv()
            total_ref[r] += from_low[z, r].astype(F32)

        @pl.when(z < n - 1)
        def _():
            downward(z, r).wait_recv()
            total_ref[r] += from_high[z, r].astype(F32)

        y_out[r * piece : (r + 1) * piece, :] = total_ref[r].astype(BF16)

    def drain(i, carry):
        slot = 2 * i + c
        for p in range(PIECES):
            @pl.when((i <= z) & (z < n - 1))
            def _():
                hop(slot, p, 0, up).wait_send()

            @pl.when((i >= z) & (z > 0))
            def _():
                hop(slot, p, 1, down).wait_send()

            hop(slot, p, 2, side).wait_send()

        across(slot).wait_send()
        out_piece(i).wait_send()

        @pl.when(i != z)
        def _():
            direct(i).wait_send()

        for r in range(HALVES * PIECES):
            @pl.when(i > z)
            def _():
                upward(i, r).wait_send()

            @pl.when(i < z)
            def _():
                downward(i, r).wait_send()

        return carry

    lax.fori_loop(0, n, drain, 0)
    for half in range(HALVES):
        for swap in swaps(half):
            swap.wait_send()


def finish_kernel(
    mem_ref, vts, kps, dfull, y_ref, k_ref, v_ref, nn_ref, ns_ref, ni_ref, nf_ref,
    nm_out, y_out, k_out, v_out, nn_out, ns_out, ni_out, nf_out,
    k_tmp, v_tmp,
):
    step = pl.program_id(0)
    block, heads, values, keys = mem_ref.shape
    _, span, width = y_out.shape
    lanes = 128

    @pl.when(step == 0)
    def _():
        nn_out[...] = nn_ref[...]
        ns_out[...] = ns_ref[...]
        ni_out[...] = ni_ref[...]
        nf_out[...] = nf_ref[...]

    y_out[...] = y_ref[...].astype(F32).reshape(block, span, width).astype(BF16)
    for src, tmp, out, size in ((k_ref, k_tmp, k_out, keys), (v_ref, v_tmp, v_out, values)):
        full = src[...].astype(F32)
        for h in range(heads):
            tmp[:, h, :] = full[:, h * size : (h + 1) * size]
        out[...] = tmp[...].reshape(block, span, heads, size).astype(BF16)

    first = step * block
    start = pl.multiple_of((first * span) // lanes * lanes, lanes)
    half = pl.ds(start, lanes)
    pair = ((iota((values, lanes), 1) + start) // span - first) // 2
    for h in range(heads):
        shared = vts[h * values : (h + 1) * values, half]
        zero = jnp.zeros_like(shared)
        left = jnp.concatenate(
            [jnp.where(pair == s, shared, zero) for s in range(block // 2)], axis=0
        )
        update = nn(left, kps[h, half, :])
        for s in range(block):
            at = s // 2 * values
            nm_out[s, h] = (
                dfull[h, pl.ds(first + s, 1), :] * mem_ref[s, h]
                + update[at : at + values, s % 2 * keys : (s % 2 + 1) * keys]
            )


def shards(
    n, tokens, norm_gain, w_query, w_key, w_value, w_outgate, w_input, w_forget, forget_bias,
    head_gain, w_out, memory, normalizer, stabilizer, prev_keys, prev_values, prev_input,
    prev_forget, accepted,
):
    seqs, span, width = tokens.shape
    depth, heads, keys = w_query.shape
    values = w_value.shape[2]
    rows = seqs * span
    hk, hv = heads * keys, heads * values
    all_heads = w_input.shape[1]
    sds = jax.ShapeDtypeStruct
    vm = pl.BlockSpec(memory_space=pltpu.VMEM)
    hbm = pl.BlockSpec(memory_space=pl.ANY)
    flip = lambda w: w.transpose(1, 2, 0).reshape(-1, depth)

    lanes = rows // HALVES
    piece = lanes // PIECES
    parts = HALVES * PIECES
    blocks = seqs // BLOCK
    hp = -(-heads // 8) * 8
    channels = 2 * hk + 2 * hv + 2 * all_heads
    dma = lambda *shape: pltpu.SemaphoreType.DMA(shape)
    y, k, v, vts, kps, dfull, new_n, ns, ni, nf = pl.pallas_call(
        functools.partial(fused_kernel, n, keys, head_gain.shape[1]),
        out_shape=[
            sds((rows, width), BF16), sds((rows, hk), BF16), sds((rows, hv), BF16),
            sds((hv, rows), BF16), sds((heads, rows, 2 * keys), BF16), sds((heads, seqs, keys), F32),
            sds(normalizer.shape, F32), sds((heads, seqs), F32),
            sds((span, heads, seqs), F32), sds((span, heads, seqs), F32),
        ],
        in_specs=[vm] * 11 + [hbm] * 8,
        out_specs=[vm] * 10,
        scratch_shapes=[
            pltpu.VMEM((2 * n, HALVES, lanes, width), BF16),
            pltpu.VMEM((channels, depth), BF16),
            pltpu.VMEM((HALVES, channels, lanes), F32),
            pltpu.VMEM((HALVES, lanes, 128), F32),
            pltpu.VMEM(memory.shape, F32),
            pltpu.VMEM((heads, seqs // 4, values, 4 * keys), BF16),
            pltpu.VMEM((heads, seqs, keys), BF16),
            pltpu.VMEM((2, hp, rows), F32),
            pltpu.VMEM((hp, rows), F32),
            pltpu.VMEM((HALVES, hv, lanes), BF16),
            pltpu.VMEM((HALVES, heads, lanes), F32),
            pltpu.VMEM((HALVES, hv, lanes), BF16),
            pltpu.VMEM((HALVES, heads, lanes), F32),
            pltpu.VMEM((rows, 2 * hv), BF16),
            pltpu.VMEM((n, 2 * hv, width), BF16),
        ]
        + [pltpu.VMEM((n, parts, piece, width), BF16)] * 4
        + [
            pltpu.VMEM((parts, piece, width), F32),
            dma(6), dma(blocks), dma(n), dma(n), dma(n),
            dma(3, 2 * n, PIECES), dma(2 * n, PIECES), dma(n), dma(2 * n), dma(2 * n),
            dma(HALVES, 2), dma(HALVES, 2),
        ]
        + [dma(n, parts)] * 4,
        compiler_params=pltpu.CompilerParams(
            collective_id=0, has_side_effects=True, vmem_limit_bytes=VMEM_LIMIT
        ),
        name="fused",
    )(
        tokens, norm_gain.reshape(1, depth), forget_bias.reshape(1, all_heads),
        prev_keys, prev_values, prev_input.transpose(1, 2, 0), prev_forget.transpose(1, 2, 0),
        accepted.reshape(1, seqs), stabilizer.T, normalizer, head_gain,
        flip(w_query), flip(w_key), flip(w_value), flip(w_outgate),
        w_input.T, w_forget.T, memory, w_out.reshape(hv, -1),
    )

    whole = lambda *shape: pl.BlockSpec(shape, lambda i: (0,) * len(shape))
    strip = lambda size: pl.BlockSpec((BLOCK * span, size), lambda i: (i, 0))
    tile = pl.BlockSpec((BLOCK, heads, values, keys), lambda i: (i, 0, 0, 0))
    fresh = lambda size: pl.BlockSpec((BLOCK, span, heads, size), lambda i: (i, 0, 0, 0))
    new_memory, y, k, v, new_n, ns, ni, nf = pl.pallas_call(
        finish_kernel,
        grid=(blocks,),
        out_shape=[
            sds(memory.shape, F32), sds(tokens.shape, BF16), sds((seqs, span, heads, keys), BF16),
            sds((seqs, span, heads, values), BF16), sds(normalizer.shape, F32),
            sds((heads, seqs), F32), sds((span, heads, seqs), F32), sds((span, heads, seqs), F32),
        ],
        in_specs=[
            tile, whole(hv, rows), whole(heads, rows, 2 * keys), whole(heads, seqs, keys),
            strip(width), strip(hk), strip(hv), whole(seqs, heads, keys), whole(heads, seqs),
            whole(span, heads, seqs), whole(span, heads, seqs),
        ],
        out_specs=[
            tile, pl.BlockSpec((BLOCK, span, width), lambda i: (i, 0, 0)), fresh(keys), fresh(values),
            whole(seqs, heads, keys), whole(heads, seqs), whole(span, heads, seqs),
            whole(span, heads, seqs),
        ],
        scratch_shapes=[
            pltpu.VMEM((BLOCK * span, heads, keys), F32),
            pltpu.VMEM((BLOCK * span, heads, values), F32),
        ],
        compiler_params=pltpu.CompilerParams(vmem_limit_bytes=VMEM_LIMIT),
        name="finish",
    )(memory, vts, kps, dfull, y, k, v, new_n, ns, ni, nf)

    return y, new_memory, new_n, ns.T, k, v, ni.transpose(2, 0, 1), nf.transpose(2, 0, 1)


def solution(mesh):
    return jax.shard_map(
        functools.partial(shards, mesh.shape["kv"]),
        mesh=mesh,
        in_specs=(
            P(("grp", "dp"), None, ("kv", "tp")),
            P(),
            P(None, "kv", None),
            P(None, "kv", None),
            P(None, "kv", "tp"),
            P(None, "kv", "tp"),
            P(),
            P(),
            P(),
            P(),
            P("kv", "tp", None),
            P(("grp", "dp"), "kv", "tp", None),
            P(("grp", "dp"), "kv", None),
            P(("grp", "dp"), "kv"),
            P(("grp", "dp"), None, "kv", None),
            P(("grp", "dp"), None, "kv", "tp"),
            P(("grp", "dp"), None, "kv"),
            P(("grp", "dp"), None, "kv"),
            P(("grp", "dp")),
        ),
        out_specs=(
            P(("grp", "dp"), None, ("kv", "tp")),
            P(("grp", "dp"), "kv", "tp", None),
            P(("grp", "dp"), "kv", None),
            P(("grp", "dp"), "kv"),
            P(("grp", "dp"), None, "kv", None),
            P(("grp", "dp"), None, "kv", "tp"),
            P(("grp", "dp"), None, "kv"),
            P(("grp", "dp"), None, "kv"),
        ),
        check_vma=False,
    )
```

```python
import functools
import jax
import jax.numpy as jnp
from jax import lax
from jax.sharding import PartitionSpec as P
from jax.experimental import pallas as pl
from jax.experimental.pallas import tpu as pltpu

EPS = 1e-06
FAR_NEGATIVE = -1e30
HIGHEST = lax.Precision.HIGHEST
MESH = pl.DeviceIdType.MESH
F32 = jnp.float32
BF16 = jnp.bfloat16
FUSED_LIMIT = 40 << 20
FINISH_LIMIT = 8 << 20
CHUNKS = (2, 2)
PIECES = 2
PIECE = 32
BLOCK = 8


def nn(a, b, precision=None):
    return lax.dot_general(
        a, b, (((1,), (0,)), ((), ())), precision=precision, preferred_element_type=F32
    )


def nt(a, b, precision=None):
    return lax.dot_general(
        a, b, (((1,), (1,)), ((), ())), precision=precision, preferred_element_type=F32
    )


def iota(shape, d):
    return lax.broadcasted_iota(jnp.int32, shape, d)


def enter(n, z, c):
    barrier = pltpu.get_barrier_semaphore()
    pl.semaphore_signal(barrier, inc=1, device_id={"tp": 1 - c}, device_id_type=MESH)

    @pl.when(z > 0)
    def _():
        pl.semaphore_signal(barrier, inc=1, device_id={"kv": z - 1}, device_id_type=MESH)

    @pl.when(z < n - 1)
    def _():
        pl.semaphore_signal(barrier, inc=1, device_id={"kv": z + 1}, device_id_type=MESH)

    peers = 1 + (z > 0).astype(jnp.int32) + (z < n - 1).astype(jnp.int32)
    pl.semaphore_wait(barrier, peers)


def fused_kernel(
    n, key_size, full_values,
    x_ref, gain_ref, bias_ref, pk_ref, pv_ref, pi_ref, pf_ref, acc_ref, stab_ref, nrm_ref, hgain_ref,
    wq_hbm, wk_hbm, wv_hbm, wo_hbm, wi_hbm, wf_hbm, mem_hbm, out_hbm,
    y_out, k_out, v_out, mem, nn_out, ns_out, ni_out, nf_out,
    xg, weights, acc, squares, vts, kps, dfull, packed, nrmb, gates, nsrow, k_all, v_all, k_tmp, v_tmp, g_own, sq_own, g_in, sq_in, both,
    w_ref, from_low, from_high, to_high, to_low, term_ref, total_ref,
    load_sem, mem_sem, wload_sem, wsend_sem, wrecv_sem,
    send0, recv0, send1, side1, recv1, ex_send, ex_recv, up_send, up_recv, down_send, down_recv,
):
    z = lax.axis_index("kv")
    c = lax.axis_index("tp")
    seqs, span, width = x_ref.shape
    rows = seqs * span
    unit = rows // sum(CHUNKS)
    chunks, start = [], 0
    for size in CHUNKS:
        chunks.append((start * unit, size * unit))
        start += size
    wide_lanes = acc.shape[2]
    piece = chunks[0][1] // PIECES
    depth = gain_ref.shape[1]
    keys = key_size
    heads, values = pv_ref.shape[2:]
    hk, hv = heads * keys, heads * values
    blocks = seqs // BLOCK
    hp = nsrow.shape[0]
    up, down, side = {"kv": z + 1}, {"kv": z - 1}, {"tp": 1 - c}

    loads, spans, at = [], [], 0
    for i, src in enumerate((wq_hbm, wk_hbm, wv_hbm, wo_hbm, wi_hbm, wf_hbm)):
        size = src.shape[0]
        spans.append(slice(at, at + size))
        loads.append(
            pltpu.make_async_copy(src, weights.at[pl.ds(at, size)], load_sem.at[i])
        )
        at += size

    def mem_load(b):
        part = pl.ds(b * BLOCK, BLOCK)
        return pltpu.make_async_copy(mem_hbm.at[part], mem.at[part], mem_sem.at[b])

    def own_load(d):
        col = pl.multiple_of((2 * d + c) * width, width)
        return pltpu.make_async_copy(
            out_hbm.at[:, pl.ds(col, width)], w_ref.at[d, pl.ds(0, hv)], wload_sem.at[d]
        )

    def out_piece(d):
        col = pl.multiple_of((2 * d + 1 - c) * width, width)
        return pltpu.make_async_remote_copy(
            src_ref=out_hbm.at[:, pl.ds(col, width)], dst_ref=w_ref.at[d, pl.ds(hv, hv)],
            send_sem=wsend_sem.at[d], recv_sem=wrecv_sem.at[d],
            device_id=side, device_id_type=MESH,
        )

    def hop(slot, p, way, target):
        part = pl.ds(p * piece, piece)
        return pltpu.make_async_remote_copy(
            src_ref=xg.at[slot, part], dst_ref=xg.at[slot, part],
            send_sem=send0.at[way, slot, p], recv_sem=recv0.at[slot, p],
            device_id=target, device_id_type=MESH,
        )

    mine = 2 * z + c

    def direct(ch, target):
        part = pl.ds(*chunks[ch])
        return pltpu.make_async_remote_copy(
            src_ref=xg.at[mine, part], dst_ref=xg.at[mine, part],
            send_sem=send1.at[ch, target], recv_sem=recv1.at[ch, mine],
            device_id={"kv": target}, device_id_type=MESH,
        )

    def across(ch, slot):
        part = pl.ds(*chunks[ch])
        return pltpu.make_async_remote_copy(
            src_ref=xg.at[slot, part], dst_ref=xg.at[slot, part],
            send_sem=side1.at[ch, slot], recv_sem=recv1.at[ch, slot],
            device_id=side, device_id_type=MESH,
        )

    for load in loads:
        load.start()
    flat = x_ref[...].reshape(rows, width)
    xg[mine] = flat
    enter(n, z, c)

    for p in range(PIECES):
        @pl.when(z < n - 1)
        def _():
            hop(mine, p, 0, up).start()

        @pl.when(z > 0)
        def _():
            hop(mine, p, 1, down).start()

    for p in range(PIECES):
        hop(mine, p, 2, side).start()
    for ch in range(1, len(chunks)):
        across(ch, mine).start()

    @pl.when(z == 0)
    def _():
        direct(1, z + 1).start()

    @pl.when(z == n - 1)
    def _():
        direct(1, z - 1).start()

    for b in range(blocks):
        mem_load(b).start()
    for d in range(n):
        own_load(d).start()
        out_piece(d).start()

    acc[...] = jnp.zeros_like(acc)
    squares[...] = jnp.zeros_like(squares)
    gates[...] = jnp.zeros_like(gates)
    g_own[...] = jnp.zeros_like(g_own)
    sq_own[...] = jnp.zeros_like(sq_own)

    expand = (iota((seqs, rows), 0) == iota((seqs, rows), 1) // span).astype(F32)
    lane_pos = iota((span, rows), 1) % span == iota((span, rows), 0)
    dropped = iota((span, seqs), 0) >= acc_ref[...]
    stack, decays, tops = [], [], []
    for h in range(heads):
        stab = stab_ref[h : h + 1, :]
        f = jnp.where(dropped, 0.0, pf_ref[:, h, :])
        i = jnp.where(dropped, FAR_NEGATIVE, pi_ref[:, h, :])
        run = []
        for j in range(span):
            run.append(f[j : j + 1] + run[-1] if run else f[0:1])
        e = run[-1]
        u = e - jnp.concatenate(run, axis=0) + i
        ns = jnp.maximum(e + stab, jnp.max(u, axis=0, keepdims=True))
        ns_out[h : h + 1, :] = ns
        tops.append(ns)
        decays.append(jnp.exp(e + stab - ns))
        stack += [jnp.exp(u - ns), jnp.zeros((8 - span, seqs), F32)]
    tops.append(jnp.zeros((hp - heads, seqs), F32))
    wide = nn(jnp.concatenate(stack, axis=0), expand, HIGHEST)
    shape = (seqs, len(chunks) * wide_lanes)
    lane = iota(shape, 1)
    padded = jnp.zeros(shape, jnp.bool_)
    for ch, (r0, m) in enumerate(chunks):
        at = lane - ch * wide_lanes
        padded = padded | ((at >= 0) & (at < m) & (iota(shape, 0) == (at + r0) // span))
    padded = padded.astype(F32)
    nsrow[...] = nn(jnp.concatenate(tops, axis=0), padded, HIGHEST)
    decays = jnp.concatenate(decays + [jnp.zeros((hp - heads, seqs), F32)], axis=0).T
    old_keys = pk_ref[...].astype(F32).reshape(rows, heads, keys)
    old_values = pv_ref[...].astype(F32).reshape(rows, heads, values)
    odd = (iota((rows, keys), 0) // span) % 2
    spread = iota((seqs, rows), 0) == iota((seqs, rows), 1) // span
    for h in range(heads):
        share_row = jnp.sum(
            jnp.where(lane_pos, wide[8 * h : 8 * h + span], 0.0), axis=0, keepdims=True
        )
        old = old_keys[:, h, :].astype(BF16)
        kps[h] = jnp.concatenate(
            [jnp.where(odd == p, old, jnp.zeros_like(old)) for p in range(2)], axis=1
        )
        part = slice(h * values, (h + 1) * values)
        vts[part, :] = (old_values[:, h, :].T * share_row).astype(BF16)
        full = jnp.broadcast_to(decays[:, h : h + 1], (seqs, keys))
        dfull[h] = full
        after = full * nrm_ref[:, h, :] + nn(jnp.where(spread, share_row, 0.0).astype(BF16), old)
        nn_out[:, h, :] = after
        nrmb[h] = after.astype(BF16)

    def remember(b):
        mem_load(b).wait()
        first = b * BLOCK
        start = pl.multiple_of((first * span) // 128 * 128, 128)
        half = pl.ds(start, 128)
        pair = ((iota((values, 128), 1) + start) // span - first) // 2
        for h in range(heads):
            shared = vts[h * values : (h + 1) * values, half]
            zero = jnp.zeros_like(shared)
            left = jnp.concatenate(
                [jnp.where(pair == s, shared, zero) for s in range(BLOCK // 2)], axis=0
            )
            update = nn(left, kps[h, half, :])
            pairs = []
            for s in range(BLOCK // 2):
                after = []
                for p in range(2):
                    seq = first + 2 * s + p
                    fresh = update[s * values : (s + 1) * values, p * keys : (p + 1) * keys]
                    after.append(dfull[h, pl.ds(seq, 1), :] * mem[seq, h] + fresh)
                    mem[seq, h] = after[p]
                pairs.append(jnp.concatenate(after, axis=1).astype(BF16))
            for s in range(BLOCK // 4):
                packed[h, b * (BLOCK // 4) + s] = jnp.concatenate(pairs[2 * s : 2 * s + 2], axis=1)

    def process(owner, ch):
        r0, m = chunks[ch]
        cols = pl.ds(pl.multiple_of(owner * 2 * width, 2 * width), 2 * width)
        x = jnp.concatenate(
            [xg[2 * owner + i, pl.ds(r0, m), :] for i in range(2)], axis=1
        ).astype(F32)
        square = x * x
        total = squares[ch, :m]
        for i in range(2 * width // 128):
            total = total + square[:, i * 128 : (i + 1) * 128]
        squares[ch, :m] = total
        acc[ch, :, :m] += nt(weights[:, cols], (x * gain_ref[:, cols]).astype(BF16))

    def process_first(owner):
        for p in range(PIECES):
            hop(2 * owner + 1 - c, p, 2, side).wait_recv()
        process(owner, 0)

    def process_later(owner, ch):
        across(ch, 2 * owner + 1 - c).wait_recv()
        process(owner, ch)

    for load in loads:
        load.wait()
    per = -(-blocks // (n - 1))

    def remember_some(k):
        for j in range(per):
            b = k * per + j

            @pl.when(b < blocks)
            def _():
                remember(b)

    process_first(z)
    remember_some(0)

    def pair(k):
        return ((z + k, z + k <= n - 1), (z - k, z - k >= 0))

    def send_later(k):
        for target, there in pair(k):
            @pl.when(there)
            def _():
                direct(1, target).start()

    def gather_first(k, carry):
        @pl.when(k > 2)
        def _():
            send_later(k - 1)

        for p in range(PIECES):
            @pl.when(z - k >= 0)
            def _():
                slot = 2 * (z - k) + c
                hop(slot, p, 0, up).wait_recv()

                @pl.when(z < n - 1)
                def _():
                    hop(slot, p, 0, up).start()

                hop(slot, p, 2, side).start()

            @pl.when(z + k <= n - 1)
            def _():
                slot = 2 * (z + k) + c
                hop(slot, p, 1, down).wait_recv()

                @pl.when(z > 0)
                def _():
                    hop(slot, p, 1, down).start()

                hop(slot, p, 2, side).start()

        @pl.when((k == z) & (z < n - 1))
        def _():
            direct(1, z + 1).start()

        @pl.when((k == n - 1 - z) & (z > 0))
        def _():
            direct(1, z - 1).start()

        @pl.when(k < n - 1)
        def _():
            remember_some(k)

            for owner, there in pair(k):
                @pl.when(there)
                def _():
                    process_first(owner)

        return carry

    lax.fori_loop(1, n, gather_first, 0)

    if n > 2:
        send_later(n - 1)
    process_later(z, 1)
    for owner, there in pair(n - 1):
        @pl.when(there)
        def _():
            process_first(owner)

    local_gain = hgain_ref[:, :values]
    for i in range(1, hgain_ref.shape[1] // values):
        local_gain = jnp.where(c == i, hgain_ref[:, i * values : (i + 1) * values], local_gain)
    gains = local_gain[:heads]
    for i in range(1, hgain_ref.shape[0] // heads):
        gains = jnp.where(z == i, local_gain[i * heads : (i + 1) * heads], gains)
    columns = jnp.concatenate([gains, jnp.zeros((hp - heads, values), F32)], axis=0).T

    def recur(ch):
        r0, lanes = chunks[ch]
        part_of = pl.ds(r0, lanes)
        padded_part = pl.ds(ch * wide_lanes, lanes)
        place = iota((hp, lanes), 1) % span
        summed = nt(jnp.ones((8, 128), F32), squares[ch, :lanes], HIGHEST)
        inv = lax.rsqrt(summed[0:1] / depth + EPS)
        q, k, v, og, gi, gf = [acc[ch, part, :lanes] * inv for part in spans]
        q = (q.astype(BF16).astype(F32) * keys ** (-0.5)).astype(BF16)
        k_rows = k.T.astype(BF16)
        v = v.astype(BF16)
        k_all[part_of, :] = k_rows
        v_all[part_of, :] = v.astype(F32).T.astype(BF16)
        all_heads = gf.shape[0]
        diagonal = iota((all_heads, all_heads), 0) == iota((all_heads, all_heads), 1)
        shift = nn(jnp.where(diagonal, bias_ref[...], 0.0), jnp.ones(gf.shape, F32), HIGHEST)
        raw = gf + shift
        gf = jnp.minimum(raw, 0.0) - jnp.log1p(jnp.exp(-jnp.abs(raw)))
        chosen = []
        for total in (gi, gf):
            out = total[:heads]
            for i in range(1, n):
                out = jnp.where(z == i, total[i * heads : (i + 1) * heads], out)
            chosen.append(jnp.concatenate([out, jnp.zeros((hp - heads, lanes), F32)], axis=0))
        inflow, run = chosen
        gates[0, :, padded_part] = inflow
        gates[1, :, padded_part] = run
        step = 1
        while step < span:
            run = run + jnp.where(place >= step, pltpu.roll(run, step, 1), 0.0)
            step *= 2
        deltas = [inflow]
        for i in range(1, span):
            spread_i = run - pltpu.roll(run, i, 1) + pltpu.roll(inflow, i, 1)
            deltas.append(jnp.where(place >= i, spread_i, FAR_NEGATIVE))
        carried = run + nsrow[:, padded_part]
        top = carried
        for d in deltas:
            top = jnp.maximum(top, d)
        scale = jnp.exp(carried - top)
        floor = jnp.exp(-top)
        ws = [jnp.exp(d - top) for d in deltas]
        placed = []
        for u in range(span):
            w = jnp.zeros_like(top)
            for i in range(span):
                w = jnp.where(place - u == i, ws[i], w)
            placed.append(w)
        same = iota((lanes, lanes), 0) // span == iota((lanes, lanes), 1) // span
        owner = iota(q.shape, 0) // keys
        count = lanes // span
        here = iota((count, lanes), 0) == iota((count, lanes), 1) // span
        quarter = (iota((keys, lanes), 1) // span) % 4
        quad = iota((values, lanes), 1) // span // 4
        for h in range(heads):
            part = slice(h * values, (h + 1) * values)
            query = q[h * keys : (h + 1) * keys]
            none = jnp.zeros_like(query)
            four = jnp.concatenate([jnp.where(quarter == p, query, none) for p in range(4)], axis=0)
            table = packed[h, r0 // span // 4 : (r0 // span + count) // 4]
            read = nn(table.reshape(count // 4 * values, 4 * keys), four)
            recalled = read[:values]
            for s in range(1, count // 4):
                recalled = jnp.where(quad == s, read[s * values : (s + 1) * values], recalled)
            only = jnp.where(owner == h, q, jnp.zeros_like(q))
            w = jnp.concatenate([placed[u][h : h + 1] for u in range(span)] * (8 // span), axis=0)
            w = jnp.broadcast_to(w[None], (lanes // 8, 8, lanes)).reshape(lanes, lanes)
            w = jnp.where(same, w * nn(k_rows, only), 0.0)
            nq = nn(nrmb[h, r0 // span : r0 // span + count], query)
            nq = jnp.sum(jnp.where(here, nq, 0.0), axis=0, keepdims=True)
            carry = scale[h : h + 1]
            over = nn(v[part], w.astype(BF16)) + carry * recalled
            under = jnp.sum(w, axis=0, keepdims=True) + carry * nq
            cell = over / jnp.maximum(jnp.abs(under), floor[h : h + 1])
            sq_own[ch, h : h + 1, :lanes] = jnp.sum(cell * cell, axis=0, keepdims=True)
            g = jax.nn.sigmoid(og[part]) * cell * columns[:, h : h + 1]
            g_own[ch, part, :lanes] = g.astype(BF16)

    def swaps(ch):
        return [
            pltpu.make_async_remote_copy(
                src_ref=src.at[ch], dst_ref=dst.at[ch],
                send_sem=ex_send.at[ch, i], recv_sem=ex_recv.at[ch, i],
                device_id=side, device_id_type=MESH,
            )
            for i, (src, dst) in enumerate(((g_own, g_in), (sq_own, sq_in)))
        ]

    def join(ch):
        r0, m = chunks[ch]
        for swap in swaps(ch):
            swap.wait_recv()
        inv = lax.rsqrt((sq_own[ch, :, :m] + sq_in[ch, :, :m]) / full_values + EPS)
        for i, src in enumerate((g_own, g_in)):
            scaled = jnp.concatenate(
                [
                    src[ch, h * values : (h + 1) * values, :m].astype(F32) * inv[h : h + 1, :]
                    for h in range(heads)
                ],
                axis=0,
            )
            both[r0 : r0 + m, i * hv : (i + 1) * hv] = scaled.T.astype(BF16)

    def partial(d, ch):
        r0, m = chunks[ch]
        return nn(both[r0 : r0 + m], w_ref[d])

    def upward(d, r):
        return pltpu.make_async_remote_copy(
            src_ref=to_high.at[d, pl.ds(r * PIECE, PIECE)],
            dst_ref=from_low.at[d, pl.ds(r * PIECE, PIECE)],
            send_sem=up_send.at[d, r], recv_sem=up_recv.at[d, r],
            device_id=up, device_id_type=MESH,
        )

    def downward(d, r):
        return pltpu.make_async_remote_copy(
            src_ref=to_low.at[d, pl.ds(r * PIECE, PIECE)],
            dst_ref=from_high.at[d, pl.ds(r * PIECE, PIECE)],
            send_sem=down_send.at[d, r], recv_sem=down_recv.at[d, r],
            device_id=down, device_id_type=MESH,
        )

    def units(ch):
        r0, m = chunks[ch]
        return range(r0 // PIECE, (r0 + m) // PIECE)

    def send_first(ch):
        r0, m = chunks[ch]

        def body(i, carry):
            @pl.when(z == 0)
            def _():
                to_high[n - 1 - i, r0 : r0 + m] = partial(n - 1 - i, ch).astype(BF16)
                for r in units(ch):
                    upward(n - 1 - i, r).start()

            @pl.when(z == n - 1)
            def _():
                to_low[i, r0 : r0 + m] = partial(i, ch).astype(BF16)
                for r in units(ch):
                    downward(i, r).start()

            return carry

        lax.fori_loop(0, n - 1, body, 0)

    def send_next(ch):
        r0, m = chunks[ch]

        def body(i, carry):
            high = n - 1 - i + z
            low = i - (n - 1 - z)
            rising = (z > 0) & (high > z) & (high <= n - 1)
            falling = (z < n - 1) & (low < z) & (low >= 0)

            @pl.when(rising)
            def _():
                term_ref[0, :m] = partial(high, ch)

            @pl.when(falling)
            def _():
                term_ref[1, :m] = partial(low, ch)

            for r in units(ch):
                at = slice(r * PIECE, (r + 1) * PIECE)
                mid = slice(r * PIECE - r0, (r + 1) * PIECE - r0)

                @pl.when(rising)
                def _():
                    upward(high, r).wait_recv()
                    to_high[high, at] = (term_ref[0, mid] + from_low[high, at].astype(F32)).astype(BF16)
                    upward(high, r).start()

                @pl.when(falling)
                def _():
                    downward(low, r).wait_recv()
                    to_low[low, at] = (term_ref[1, mid] + from_high[low, at].astype(F32)).astype(BF16)
                    downward(low, r).start()

            return carry

        lax.fori_loop(0, 2 * n - 2, body, 0)

    def arrive(ch, k):
        for slot, there in ((2 * (z - k) + c, z - k >= 0), (2 * (z + k) + c, z + k <= n - 1)):
            @pl.when(there)
            def _():
                across(ch, slot).wait_recv()
                across(ch, slot).start()

    def work(ch, k):
        for owner, there in ((z - k, z - k >= 0), (z + k, z + k <= n - 1)):
            @pl.when(there)
            def _():
                process_later(owner, ch)

    recur(0)
    for swap in swaps(0):
        swap.start()
    arrive(1, 1)
    for d in range(n):
        own_load(d).wait()
        out_piece(d).wait_recv()
    join(0)
    send_first(0)
    work(1, 1)

    def gather_later(k, carry):
        arrive(1, k)

        @pl.when(k > 2)
        def _():
            work(1, k - 1)

        return carry

    lax.fori_loop(2, n, gather_later, 0)
    work(1, n - 1)
    recur(1)
    for swap in swaps(1):
        swap.start()
    join(1)
    send_first(1)
    send_next(0)
    send_next(1)

    total_ref[...] = nn(both[...], w_ref[z])
    for src, tmp, out, size in ((k_all, k_tmp, k_out, keys), (v_all, v_tmp, v_out, values)):
        full = src[...].astype(F32)
        for h in range(heads):
            tmp[:, h, :] = full[:, h * size : (h + 1) * size]
        out[...] = tmp[...].reshape(seqs, span, heads, size).astype(BF16)
    pos = iota((span, len(chunks) * wide_lanes), 1) % span
    lane_pos = pos == iota((span, len(chunks) * wide_lanes), 0)
    single = [
        jnp.where(lane_pos, gates[i, h : h + 1, :], 0.0) for h in range(heads) for i in range(2)
    ]
    compact = nt(jnp.concatenate(single, axis=0), padded, HIGHEST)
    for h in range(heads):
        ni_out[:, h, :] = compact[2 * h * span : (2 * h + 1) * span]
        nf_out[:, h, :] = compact[(2 * h + 1) * span : (2 * h + 2) * span]
    for r in range(rows // PIECE):
        at = slice(r * PIECE, (r + 1) * PIECE)

        @pl.when(z > 0)
        def _():
            upward(z, r).wait_recv()
            total_ref[at] += from_low[z, at].astype(F32)

        @pl.when(z < n - 1)
        def _():
            downward(z, r).wait_recv()
            total_ref[at] += from_high[z, at].astype(F32)

        count = PIECE // span
        y_out[r * count : (r + 1) * count] = total_ref[at].reshape(count, span, width).astype(BF16)

    def drain(i, carry):
        slot = 2 * i + c
        for p in range(PIECES):
            @pl.when((i <= z) & (z < n - 1))
            def _():
                hop(slot, p, 0, up).wait_send()

            @pl.when((i >= z) & (z > 0))
            def _():
                hop(slot, p, 1, down).wait_send()

            hop(slot, p, 2, side).wait_send()

        out_piece(i).wait_send()
        for ch in range(1, len(chunks)):
            across(ch, slot).wait_send()

            @pl.when(i != z)
            def _():
                direct(ch, i).wait_send()

        for r in range(rows // PIECE):
            @pl.when(i > z)
            def _():
                upward(i, r).wait_send()

            @pl.when(i < z)
            def _():
                downward(i, r).wait_send()

        return carry

    lax.fori_loop(0, n, drain, 0)
    for ch in range(len(chunks)):
        for swap in swaps(ch):
            swap.wait_send()


def finish_kernel(*refs):
    count = (len(refs) - 1) // 2
    sem = refs[-1]
    copies = [
        pltpu.make_async_copy(src, dst, sem.at[i])
        for i, (src, dst) in enumerate(zip(refs[1:count], refs[count + 1 : 2 * count]))
    ]
    memory, new_memory = refs[0], refs[count]
    for b in range(memory.shape[0] // BLOCK):
        part = pl.ds(b * BLOCK, BLOCK)
        copies.append(
            pltpu.make_async_copy(memory.at[part], new_memory.at[part], sem.at[count - 1 + b])
        )
    for copy in copies:
        copy.start()
    for copy in copies:
        copy.wait()


def shards(
    n, tokens, norm_gain, w_query, w_key, w_value, w_outgate, w_input, w_forget, forget_bias,
    head_gain, w_out, memory, normalizer, stabilizer, prev_keys, prev_values, prev_input,
    prev_forget, accepted,
):
    seqs, span, width = tokens.shape
    depth, heads, keys = w_query.shape
    values = w_value.shape[2]
    rows = seqs * span
    hk, hv = heads * keys, heads * values
    all_heads = w_input.shape[1]
    sds = jax.ShapeDtypeStruct
    vm = pl.BlockSpec(memory_space=pltpu.VMEM)
    hbm = pl.BlockSpec(memory_space=pl.ANY)
    flip = lambda w: w.transpose(1, 2, 0).reshape(-1, depth)

    parts = sum(CHUNKS)
    unit = rows // parts
    lanes = -(-unit * max(CHUNKS) // 128) * 128
    count = len(CHUNKS)
    blocks = seqs // BLOCK
    hp = -(-heads // 8) * 8
    channels = 2 * hk + 2 * hv + 2 * all_heads
    dma = lambda *shape: pltpu.SemaphoreType.DMA(shape)
    outs = [
        sds(tokens.shape, BF16), sds((seqs, span, heads, keys), BF16),
        sds((seqs, span, heads, values), BF16), sds(memory.shape, F32),
        sds(normalizer.shape, F32), sds((heads, seqs), F32),
        sds((span, heads, seqs), F32), sds((span, heads, seqs), F32),
    ]
    y, k, v, mem, new_n, ns, ni, nf = pl.pallas_call(
        functools.partial(fused_kernel, n, keys, head_gain.shape[1]),
        out_shape=outs,
        in_specs=[vm] * 11 + [hbm] * 8,
        out_specs=[vm] * 8,
        scratch_shapes=[
            pltpu.VMEM((2 * n, rows, width), BF16),
            pltpu.VMEM((channels, depth), BF16),
            pltpu.VMEM((count, channels, lanes), F32),
            pltpu.VMEM((count, lanes, 128), F32),
            pltpu.VMEM((hv, rows), BF16),
            pltpu.VMEM((heads, rows, 2 * keys), BF16),
            pltpu.VMEM((heads, seqs, keys), F32),
            pltpu.VMEM((heads, seqs // 4, values, 4 * keys), BF16),
            pltpu.VMEM((heads, seqs, keys), BF16),
            pltpu.VMEM((2, hp, count * lanes), F32),
            pltpu.VMEM((hp, count * lanes), F32),
            pltpu.VMEM((rows, hk), BF16),
            pltpu.VMEM((rows, hv), BF16),
            pltpu.VMEM((rows, heads, keys), F32),
            pltpu.VMEM((rows, heads, values), F32),
            pltpu.VMEM((count, hv, lanes), BF16),
            pltpu.VMEM((count, heads, lanes), F32),
            pltpu.VMEM((count, hv, lanes), BF16),
            pltpu.VMEM((count, heads, lanes), F32),
            pltpu.VMEM((rows, 2 * hv), BF16),
            pltpu.VMEM((n, 2 * hv, width), BF16),
        ]
        + [pltpu.VMEM((n, rows, width), BF16)] * 4
        + [
            pltpu.VMEM((2, lanes, width), F32), pltpu.VMEM((rows, width), F32),
            dma(6), dma(blocks), dma(n), dma(n), dma(n),
            dma(3, 2 * n, PIECES), dma(2 * n, PIECES), dma(count, n), dma(count, 2 * n),
            dma(count, 2 * n), dma(count, 2), dma(count, 2),
        ]
        + [dma(n, rows // PIECE)] * 4,
        compiler_params=pltpu.CompilerParams(
            collective_id=0, has_side_effects=True, vmem_limit_bytes=FUSED_LIMIT
        ),
        name="fused",
    )(
        *[
            pltpu.with_memory_space_constraint(a, pltpu.HBM)
            for a in (
                tokens, norm_gain.reshape(1, depth), forget_bias.reshape(1, all_heads),
                prev_keys, prev_values, prev_input.transpose(1, 2, 0),
                prev_forget.transpose(1, 2, 0), accepted.reshape(1, seqs), stabilizer.T,
                normalizer, head_gain,
                flip(w_query), flip(w_key), flip(w_value), flip(w_outgate),
                w_input.T, w_forget.T, memory, w_out.reshape(hv, -1),
            )
        ]
    )

    new_memory, y, k, v, new_n, ns, ni, nf = pl.pallas_call(
        finish_kernel,
        out_shape=[outs[3], *outs[:3], *outs[4:]],
        in_specs=[vm] * 8,
        out_specs=[hbm] * 8,
        scratch_shapes=[dma(7 + blocks)],
        compiler_params=pltpu.CompilerParams(vmem_limit_bytes=FINISH_LIMIT),
        name="finish",
    )(mem, y, k, v, new_n, ns, ni, nf)

    return y, new_memory, new_n, ns.T, k, v, ni.transpose(2, 0, 1), nf.transpose(2, 0, 1)


def solution(mesh):
    return jax.shard_map(
        functools.partial(shards, mesh.shape["kv"]),
        mesh=mesh,
        in_specs=(
            P(("grp", "dp"), None, ("kv", "tp")),
            P(),
            P(None, "kv", None),
            P(None, "kv", None),
            P(None, "kv", "tp"),
            P(None, "kv", "tp"),
            P(),
            P(),
            P(),
            P(),
            P("kv", "tp", None),
            P(("grp", "dp"), "kv", "tp", None),
            P(("grp", "dp"), "kv", None),
            P(("grp", "dp"), "kv"),
            P(("grp", "dp"), None, "kv", None),
            P(("grp", "dp"), None, "kv", "tp"),
            P(("grp", "dp"), None, "kv"),
            P(("grp", "dp"), None, "kv"),
            P(("grp", "dp")),
        ),
        out_specs=(
            P(("grp", "dp"), None, ("kv", "tp")),
            P(("grp", "dp"), "kv", "tp", None),
            P(("grp", "dp"), "kv", None),
            P(("grp", "dp"), "kv"),
            P(("grp", "dp"), None, "kv", None),
            P(("grp", "dp"), None, "kv", "tp"),
            P(("grp", "dp"), None, "kv"),
            P(("grp", "dp"), None, "kv"),
        ),
        check_vma=False,
    )
```

```python
import functools
import jax
import jax.numpy as jnp
from jax import lax
from jax.sharding import PartitionSpec as P
from jax.experimental import pallas as pl
from jax.experimental.pallas import tpu as pltpu

EPS = 1e-06
FAR_NEGATIVE = -1e30
HIGHEST = lax.Precision.HIGHEST
MESH = pl.DeviceIdType.MESH
F32 = jnp.float32
BF16 = jnp.bfloat16
FUSED_LIMIT = 40 << 20
FINISH_LIMIT = 8 << 20
CHUNKS = (2, 2)
PIECES = 2
PIECE = 32
BLOCK = 8


def nn(a, b, precision=None):
    return lax.dot_general(
        a, b, (((1,), (0,)), ((), ())), precision=precision, preferred_element_type=F32
    )


def nt(a, b, precision=None):
    return lax.dot_general(
        a, b, (((1,), (1,)), ((), ())), precision=precision, preferred_element_type=F32
    )


def iota(shape, d):
    return lax.broadcasted_iota(jnp.int32, shape, d)


def enter(n, z, c):
    barrier = pltpu.get_barrier_semaphore()
    pl.semaphore_signal(barrier, inc=1, device_id={"tp": 1 - c}, device_id_type=MESH)

    @pl.when(z > 0)
    def _():
        pl.semaphore_signal(barrier, inc=1, device_id={"kv": z - 1}, device_id_type=MESH)

    @pl.when(z < n - 1)
    def _():
        pl.semaphore_signal(barrier, inc=1, device_id={"kv": z + 1}, device_id_type=MESH)

    peers = 1 + (z > 0).astype(jnp.int32) + (z < n - 1).astype(jnp.int32)
    pl.semaphore_wait(barrier, peers)


def fused_kernel(
    n, key_size, full_values,
    x_ref, gain_ref, bias_ref, pk_ref, pv_ref, pi_ref, pf_ref, acc_ref, stab_ref, nrm_ref, hgain_ref,
    wq_hbm, wk_hbm, wv_hbm, wo_hbm, wi_hbm, wf_hbm, mem_hbm, out_hbm,
    y_out, k_out, v_out, mem, nn_out, ns_out, ni_out, nf_out,
    xg, weights, acc, squares, vts, kps, dfull, packed, nrmb, gates, nsrow, k_all, v_all, k_tmp, v_tmp, g_own, sq_own, g_in, sq_in, both,
    w_ref, from_low, from_high, to_high, to_low, term_ref, total_ref,
    load_sem, mem_sem, wload_sem, wsend_sem, wrecv_sem,
    send0, recv0, send1, side1, recv1, ex_send, ex_recv, up_send, up_recv, down_send, down_recv,
):
    z = lax.axis_index("kv")
    c = lax.axis_index("tp")
    seqs, span, width = x_ref.shape
    rows = seqs * span
    unit = rows // sum(CHUNKS)
    chunks, start = [], 0
    for size in CHUNKS:
        chunks.append((start * unit, size * unit))
        start += size
    wide_lanes = acc.shape[2]
    piece = chunks[0][1] // PIECES
    depth = gain_ref.shape[1]
    keys = key_size
    heads, values = pv_ref.shape[2:]
    hk, hv = heads * keys, heads * values
    blocks = seqs // BLOCK
    hp = nsrow.shape[0]
    up, down, side = {"kv": z + 1}, {"kv": z - 1}, {"tp": 1 - c}

    loads, spans, at = [], [], 0
    for i, src in enumerate((wq_hbm, wk_hbm, wv_hbm, wo_hbm, wi_hbm, wf_hbm)):
        size = src.shape[0]
        spans.append(slice(at, at + size))
        loads.append(
            pltpu.make_async_copy(src, weights.at[pl.ds(at, size)], load_sem.at[i])
        )
        at += size

    def mem_load(b):
        part = pl.ds(b * BLOCK, BLOCK)
        return pltpu.make_async_copy(mem_hbm.at[part], mem.at[part], mem_sem.at[b])

    def own_load(d):
        col = pl.multiple_of((2 * d + c) * width, width)
        return pltpu.make_async_copy(
            out_hbm.at[:, pl.ds(col, width)], w_ref.at[d, pl.ds(0, hv)], wload_sem.at[d]
        )

    def out_piece(d):
        col = pl.multiple_of((2 * d + 1 - c) * width, width)
        return pltpu.make_async_remote_copy(
            src_ref=out_hbm.at[:, pl.ds(col, width)], dst_ref=w_ref.at[d, pl.ds(hv, hv)],
            send_sem=wsend_sem.at[d], recv_sem=wrecv_sem.at[d],
            device_id=side, device_id_type=MESH,
        )

    def hop(slot, p, way, target):
        part = pl.ds(p * piece, piece)
        return pltpu.make_async_remote_copy(
            src_ref=xg.at[slot, part], dst_ref=xg.at[slot, part],
            send_sem=send0.at[way, slot, p], recv_sem=recv0.at[slot, p],
            device_id=target, device_id_type=MESH,
        )

    mine = 2 * z + c

    def direct(ch, target):
        part = pl.ds(*chunks[ch])
        return pltpu.make_async_remote_copy(
            src_ref=xg.at[mine, part], dst_ref=xg.at[mine, part],
            send_sem=send1.at[ch, target], recv_sem=recv1.at[ch, mine],
            device_id={"kv": target}, device_id_type=MESH,
        )

    def across(ch, slot):
        part = pl.ds(*chunks[ch])
        return pltpu.make_async_remote_copy(
            src_ref=xg.at[slot, part], dst_ref=xg.at[slot, part],
            send_sem=side1.at[ch, slot], recv_sem=recv1.at[ch, slot],
            device_id=side, device_id_type=MESH,
        )

    for load in loads:
        load.start()
    flat = x_ref[...].reshape(rows, width)
    xg[mine] = flat
    enter(n, z, c)

    for p in range(PIECES):
        @pl.when(z < n - 1)
        def _():
            hop(mine, p, 0, up).start()

        @pl.when(z > 0)
        def _():
            hop(mine, p, 1, down).start()

    for p in range(PIECES):
        hop(mine, p, 2, side).start()
    for ch in range(1, len(chunks)):
        across(ch, mine).start()

    @pl.when(z == 0)
    def _():
        direct(1, z + 1).start()

    @pl.when(z == n - 1)
    def _():
        direct(1, z - 1).start()

    for b in range(blocks):
        mem_load(b).start()
    for d in range(n):
        own_load(d).start()
        out_piece(d).start()

    acc[...] = jnp.zeros_like(acc)
    squares[...] = jnp.zeros_like(squares)
    gates[...] = jnp.zeros_like(gates)
    g_own[...] = jnp.zeros_like(g_own)
    sq_own[...] = jnp.zeros_like(sq_own)

    expand = (iota((seqs, rows), 0) == iota((seqs, rows), 1) // span).astype(F32)
    lane_pos = iota((span, rows), 1) % span == iota((span, rows), 0)
    dropped = iota((span, seqs), 0) >= acc_ref[...]
    stack, decays, tops = [], [], []
    for h in range(heads):
        stab = stab_ref[h : h + 1, :]
        f = jnp.where(dropped, 0.0, pf_ref[:, h, :])
        i = jnp.where(dropped, FAR_NEGATIVE, pi_ref[:, h, :])
        run = []
        for j in range(span):
            run.append(f[j : j + 1] + run[-1] if run else f[0:1])
        e = run[-1]
        u = e - jnp.concatenate(run, axis=0) + i
        ns = jnp.maximum(e + stab, jnp.max(u, axis=0, keepdims=True))
        ns_out[h : h + 1, :] = ns
        tops.append(ns)
        decays.append(jnp.exp(e + stab - ns))
        stack += [jnp.exp(u - ns), jnp.zeros((8 - span, seqs), F32)]
    tops.append(jnp.zeros((hp - heads, seqs), F32))
    wide = nn(jnp.concatenate(stack, axis=0), expand, HIGHEST)
    shape = (seqs, len(chunks) * wide_lanes)
    lane = iota(shape, 1)
    padded = jnp.zeros(shape, jnp.bool_)
    for ch, (r0, m) in enumerate(chunks):
        at = lane - ch * wide_lanes
        padded = padded | ((at >= 0) & (at < m) & (iota(shape, 0) == (at + r0) // span))
    padded = padded.astype(F32)
    nsrow[...] = nn(jnp.concatenate(tops, axis=0), padded, HIGHEST)
    decays = jnp.concatenate(decays + [jnp.zeros((hp - heads, seqs), F32)], axis=0).T
    old_keys = pk_ref[...].astype(F32).reshape(rows, heads, keys)
    old_values = pv_ref[...].astype(F32).reshape(rows, heads, values)
    odd = (iota((rows, keys), 0) // span) % 2
    spread = iota((seqs, rows), 0) == iota((seqs, rows), 1) // span
    for h in range(heads):
        share_row = jnp.sum(
            jnp.where(lane_pos, wide[8 * h : 8 * h + span], 0.0), axis=0, keepdims=True
        )
        old = old_keys[:, h, :].astype(BF16)
        kps[h] = jnp.concatenate(
            [jnp.where(odd == p, old, jnp.zeros_like(old)) for p in range(2)], axis=1
        )
        part = slice(h * values, (h + 1) * values)
        vts[part, :] = (old_values[:, h, :].T * share_row).astype(BF16)
        full = jnp.broadcast_to(decays[:, h : h + 1], (seqs, keys))
        dfull[h] = full
        after = full * nrm_ref[:, h, :] + nn(jnp.where(spread, share_row, 0.0).astype(BF16), old)
        nn_out[:, h, :] = after
        nrmb[h] = after.astype(BF16)

    def remember(b):
        mem_load(b).wait()
        first = b * BLOCK
        start = pl.multiple_of((first * span) // 128 * 128, 128)
        half = pl.ds(start, 128)
        pair = ((iota((values, 128), 1) + start) // span - first) // 2
        for h in range(heads):
            shared = vts[h * values : (h + 1) * values, half]
            zero = jnp.zeros_like(shared)
            left = jnp.concatenate(
                [jnp.where(pair == s, shared, zero) for s in range(BLOCK // 2)], axis=0
            )
            update = nn(left, kps[h, half, :])
            pairs = []
            for s in range(BLOCK // 2):
                after = []
                for p in range(2):
                    seq = first + 2 * s + p
                    fresh = update[s * values : (s + 1) * values, p * keys : (p + 1) * keys]
                    after.append(dfull[h, pl.ds(seq, 1), :] * mem[seq, h] + fresh)
                    mem[seq, h] = after[p]
                pairs.append(jnp.concatenate(after, axis=1).astype(BF16))
            for s in range(BLOCK // 4):
                packed[h, b * (BLOCK // 4) + s] = jnp.concatenate(pairs[2 * s : 2 * s + 2], axis=1)

    def process(owner, ch):
        r0, m = chunks[ch]
        cols = pl.ds(pl.multiple_of(owner * 2 * width, 2 * width), 2 * width)
        x = jnp.concatenate(
            [xg[2 * owner + i, pl.ds(r0, m), :] for i in range(2)], axis=1
        ).astype(F32)
        square = x * x
        total = squares[ch, :m]
        for i in range(2 * width // 128):
            total = total + square[:, i * 128 : (i + 1) * 128]
        squares[ch, :m] = total
        acc[ch, :, :m] += nt(weights[:, cols], (x * gain_ref[:, cols]).astype(BF16))

    def process_first(owner):
        for p in range(PIECES):
            hop(2 * owner + 1 - c, p, 2, side).wait_recv()
        process(owner, 0)

    def process_later(owner, ch):
        across(ch, 2 * owner + 1 - c).wait_recv()
        process(owner, ch)

    for load in loads:
        load.wait()
    per = -(-blocks // (n - 1))

    def remember_some(k):
        for j in range(per):
            b = k * per + j

            @pl.when(b < blocks)
            def _():
                remember(b)

    process_first(z)
    remember_some(0)

    def pair(k):
        return ((z + k, z + k <= n - 1), (z - k, z - k >= 0))

    def send_later(k):
        for target, there in pair(k):
            @pl.when(there)
            def _():
                direct(1, target).start()

    def gather_first(k, carry):
        @pl.when(k > 2)
        def _():
            send_later(k - 1)

        for p in range(PIECES):
            @pl.when(z - k >= 0)
            def _():
                slot = 2 * (z - k) + c
                hop(slot, p, 0, up).wait_recv()

                @pl.when(z < n - 1)
                def _():
                    hop(slot, p, 0, up).start()

                hop(slot, p, 2, side).start()

            @pl.when(z + k <= n - 1)
            def _():
                slot = 2 * (z + k) + c
                hop(slot, p, 1, down).wait_recv()

                @pl.when(z > 0)
                def _():
                    hop(slot, p, 1, down).start()

                hop(slot, p, 2, side).start()

        @pl.when((k == z) & (z < n - 1))
        def _():
            direct(1, z + 1).start()

        @pl.when((k == n - 1 - z) & (z > 0))
        def _():
            direct(1, z - 1).start()

        @pl.when(k < n - 1)
        def _():
            remember_some(k)

            for owner, there in pair(k):
                @pl.when(there)
                def _():
                    process_first(owner)

        return carry

    lax.fori_loop(1, n, gather_first, 0)

    if n > 2:
        send_later(n - 1)
    process_later(z, 1)
    for owner, there in pair(n - 1):
        @pl.when(there)
        def _():
            process_first(owner)

    local_gain = hgain_ref[:, :values]
    for i in range(1, hgain_ref.shape[1] // values):
        local_gain = jnp.where(c == i, hgain_ref[:, i * values : (i + 1) * values], local_gain)
    gains = local_gain[:heads]
    for i in range(1, hgain_ref.shape[0] // heads):
        gains = jnp.where(z == i, local_gain[i * heads : (i + 1) * heads], gains)
    columns = jnp.concatenate([gains, jnp.zeros((hp - heads, values), F32)], axis=0).T

    def recur(ch):
        r0, lanes = chunks[ch]
        part_of = pl.ds(r0, lanes)
        padded_part = pl.ds(ch * wide_lanes, lanes)
        place = iota((hp, lanes), 1) % span
        summed = nt(jnp.ones((8, 128), F32), squares[ch, :lanes], HIGHEST)
        inv = lax.rsqrt(summed[0:1] / depth + EPS)
        q, k, v, og, gi, gf = [acc[ch, part, :lanes] * inv for part in spans]
        q = (q.astype(BF16).astype(F32) * keys ** (-0.5)).astype(BF16)
        k_rows = k.T.astype(BF16)
        v = v.astype(BF16)
        k_all[part_of, :] = k_rows
        v_all[part_of, :] = v.astype(F32).T.astype(BF16)
        all_heads = gf.shape[0]
        diagonal = iota((all_heads, all_heads), 0) == iota((all_heads, all_heads), 1)
        shift = nn(jnp.where(diagonal, bias_ref[...], 0.0), jnp.ones(gf.shape, F32), HIGHEST)
        raw = gf + shift
        gf = jnp.minimum(raw, 0.0) - jnp.log1p(jnp.exp(-jnp.abs(raw)))
        chosen = []
        for total in (gi, gf):
            out = total[:heads]
            for i in range(1, n):
                out = jnp.where(z == i, total[i * heads : (i + 1) * heads], out)
            chosen.append(jnp.concatenate([out, jnp.zeros((hp - heads, lanes), F32)], axis=0))
        inflow, run = chosen
        gates[0, :, padded_part] = inflow
        gates[1, :, padded_part] = run
        step = 1
        while step < span:
            run = run + jnp.where(place >= step, pltpu.roll(run, step, 1), 0.0)
            step *= 2
        deltas = [inflow]
        for i in range(1, span):
            spread_i = run - pltpu.roll(run, i, 1) + pltpu.roll(inflow, i, 1)
            deltas.append(jnp.where(place >= i, spread_i, FAR_NEGATIVE))
        carried = run + nsrow[:, padded_part]
        top = carried
        for d in deltas:
            top = jnp.maximum(top, d)
        scale = jnp.exp(carried - top)
        floor = jnp.exp(-top)
        ws = [jnp.exp(d - top) for d in deltas]
        placed = []
        for u in range(span):
            w = jnp.zeros_like(top)
            for i in range(span):
                w = jnp.where(place - u == i, ws[i], w)
            placed.append(w)
        same = iota((lanes, lanes), 0) // span == iota((lanes, lanes), 1) // span
        owner = iota(q.shape, 0) // keys
        count = lanes // span
        here = iota((count, lanes), 0) == iota((count, lanes), 1) // span
        quarter = (iota((keys, lanes), 1) // span) % 4
        quad = iota((values, lanes), 1) // span // 4
        for h in range(heads):
            part = slice(h * values, (h + 1) * values)
            query = q[h * keys : (h + 1) * keys]
            none = jnp.zeros_like(query)
            four = jnp.concatenate([jnp.where(quarter == p, query, none) for p in range(4)], axis=0)
            table = packed[h, r0 // span // 4 : (r0 // span + count) // 4]
            read = nn(table.reshape(count // 4 * values, 4 * keys), four)
            recalled = read[:values]
            for s in range(1, count // 4):
                recalled = jnp.where(quad == s, read[s * values : (s + 1) * values], recalled)
            only = jnp.where(owner == h, q, jnp.zeros_like(q))
            w = jnp.concatenate([placed[u][h : h + 1] for u in range(span)] * (8 // span), axis=0)
            w = jnp.broadcast_to(w[None], (lanes // 8, 8, lanes)).reshape(lanes, lanes)
            w = jnp.where(same, w * nn(k_rows, only), 0.0)
            nq = nn(nrmb[h, r0 // span : r0 // span + count], query)
            nq = jnp.sum(jnp.where(here, nq, 0.0), axis=0, keepdims=True)
            carry = scale[h : h + 1]
            over = nn(v[part], w.astype(BF16)) + carry * recalled
            under = jnp.sum(w, axis=0, keepdims=True) + carry * nq
            cell = over / jnp.maximum(jnp.abs(under), floor[h : h + 1])
            sq_own[ch, h : h + 1, :lanes] = jnp.sum(cell * cell, axis=0, keepdims=True)
            g = jax.nn.sigmoid(og[part]) * cell * columns[:, h : h + 1]
            g_own[ch, part, :lanes] = g.astype(BF16)

    def swaps(ch):
        return [
            pltpu.make_async_remote_copy(
                src_ref=src.at[ch], dst_ref=dst.at[ch],
                send_sem=ex_send.at[ch, i], recv_sem=ex_recv.at[ch, i],
                device_id=side, device_id_type=MESH,
            )
            for i, (src, dst) in enumerate(((g_own, g_in), (sq_own, sq_in)))
        ]

    def join(ch):
        r0, m = chunks[ch]
        for swap in swaps(ch):
            swap.wait_recv()
        inv = lax.rsqrt((sq_own[ch, :, :m] + sq_in[ch, :, :m]) / full_values + EPS)
        for i, src in enumerate((g_own, g_in)):
            scaled = jnp.concatenate(
                [
                    src[ch, h * values : (h + 1) * values, :m].astype(F32) * inv[h : h + 1, :]
                    for h in range(heads)
                ],
                axis=0,
            )
            both[r0 : r0 + m, i * hv : (i + 1) * hv] = scaled.T.astype(BF16)

    def partial(d, ch):
        r0, m = chunks[ch]
        return nn(both[r0 : r0 + m], w_ref[d])

    def upward(d, r):
        return pltpu.make_async_remote_copy(
            src_ref=to_high.at[d, pl.ds(r * PIECE, PIECE)],
            dst_ref=from_low.at[d, pl.ds(r * PIECE, PIECE)],
            send_sem=up_send.at[d, r], recv_sem=up_recv.at[d, r],
            device_id=up, device_id_type=MESH,
        )

    def downward(d, r):
        return pltpu.make_async_remote_copy(
            src_ref=to_low.at[d, pl.ds(r * PIECE, PIECE)],
            dst_ref=from_high.at[d, pl.ds(r * PIECE, PIECE)],
            send_sem=down_send.at[d, r], recv_sem=down_recv.at[d, r],
            device_id=down, device_id_type=MESH,
        )

    def units(ch):
        r0, m = chunks[ch]
        return range(r0 // PIECE, (r0 + m) // PIECE)

    def send_first(ch):
        r0, m = chunks[ch]

        def body(i, carry):
            @pl.when(z == 0)
            def _():
                to_high[n - 1 - i, r0 : r0 + m] = partial(n - 1 - i, ch).astype(BF16)
                for r in units(ch):
                    upward(n - 1 - i, r).start()

            @pl.when(z == n - 1)
            def _():
                to_low[i, r0 : r0 + m] = partial(i, ch).astype(BF16)
                for r in units(ch):
                    downward(i, r).start()

            return carry

        lax.fori_loop(0, n - 1, body, 0)

    def send_next(ch):
        r0, m = chunks[ch]

        def body(i, carry):
            high = n - 1 - i + z
            low = i - (n - 1 - z)
            rising = (z > 0) & (high > z) & (high <= n - 1)
            falling = (z < n - 1) & (low < z) & (low >= 0)

            @pl.when(rising)
            def _():
                term_ref[0, :m] = partial(high, ch)

            @pl.when(falling)
            def _():
                term_ref[1, :m] = partial(low, ch)

            for r in units(ch):
                at = slice(r * PIECE, (r + 1) * PIECE)
                mid = slice(r * PIECE - r0, (r + 1) * PIECE - r0)

                @pl.when(falling)
                def _():
                    downward(low, r).wait_recv()
                    to_low[low, at] = (term_ref[1, mid] + from_high[low, at].astype(F32)).astype(BF16)
                    downward(low, r).start()

                @pl.when(rising)
                def _():
                    upward(high, r).wait_recv()
                    to_high[high, at] = (term_ref[0, mid] + from_low[high, at].astype(F32)).astype(BF16)
                    upward(high, r).start()

            return carry

        lax.fori_loop(0, 2 * n - 2, body, 0)

    def arrive(ch, k):
        for slot, there in ((2 * (z - k) + c, z - k >= 0), (2 * (z + k) + c, z + k <= n - 1)):
            @pl.when(there)
            def _():
                across(ch, slot).wait_recv()
                across(ch, slot).start()

    def work(ch, k):
        for owner, there in ((z - k, z - k >= 0), (z + k, z + k <= n - 1)):
            @pl.when(there)
            def _():
                process_later(owner, ch)

    def settle():
        for src, tmp, out, size in ((k_all, k_tmp, k_out, keys), (v_all, v_tmp, v_out, values)):
            full = src[...].astype(F32)
            for h in range(heads):
                tmp[:, h, :] = full[:, h * size : (h + 1) * size]
            out[...] = tmp[...].reshape(seqs, span, heads, size).astype(BF16)

    early = (c == 1) & ((z == 0) | (z == n - 1))

    recur(0)
    for swap in swaps(0):
        swap.start()
    arrive(1, 1)
    for d in range(n):
        own_load(d).wait()
        out_piece(d).wait_recv()
    join(0)
    send_first(0)
    work(1, 1)

    def gather_later(k, carry):
        arrive(1, k)

        @pl.when(k > 2)
        def _():
            work(1, k - 1)

        return carry

    lax.fori_loop(2, n, gather_later, 0)
    work(1, n - 1)
    recur(1)
    for swap in swaps(1):
        swap.start()
    join(1)

    @pl.when(early)
    def _():
        settle()

    send_first(1)
    send_next(0)
    send_next(1)

    total_ref[...] = nn(both[...], w_ref[z])
    @pl.when(jnp.logical_not(early))
    def _():
        settle()

    pos = iota((span, len(chunks) * wide_lanes), 1) % span
    lane_pos = pos == iota((span, len(chunks) * wide_lanes), 0)
    single = [
        jnp.where(lane_pos, gates[i, h : h + 1, :], 0.0) for h in range(heads) for i in range(2)
    ]
    compact = nt(jnp.concatenate(single, axis=0), padded, HIGHEST)
    for h in range(heads):
        ni_out[:, h, :] = compact[2 * h * span : (2 * h + 1) * span]
        nf_out[:, h, :] = compact[(2 * h + 1) * span : (2 * h + 2) * span]
    for r in range(rows // PIECE):
        at = slice(r * PIECE, (r + 1) * PIECE)

        @pl.when(z > 0)
        def _():
            upward(z, r).wait_recv()
            total_ref[at] += from_low[z, at].astype(F32)

        @pl.when(z < n - 1)
        def _():
            downward(z, r).wait_recv()
            total_ref[at] += from_high[z, at].astype(F32)

        count = PIECE // span
        y_out[r * count : (r + 1) * count] = total_ref[at].reshape(count, span, width).astype(BF16)

    def drain(i, carry):
        slot = 2 * i + c
        for p in range(PIECES):
            @pl.when((i <= z) & (z < n - 1))
            def _():
                hop(slot, p, 0, up).wait_send()

            @pl.when((i >= z) & (z > 0))
            def _():
                hop(slot, p, 1, down).wait_send()

            hop(slot, p, 2, side).wait_send()

        out_piece(i).wait_send()
        for ch in range(1, len(chunks)):
            across(ch, slot).wait_send()

            @pl.when(i != z)
            def _():
                direct(ch, i).wait_send()

        for r in range(rows // PIECE):
            @pl.when(i > z)
            def _():
                upward(i, r).wait_send()

            @pl.when(i < z)
            def _():
                downward(i, r).wait_send()

        return carry

    lax.fori_loop(0, n, drain, 0)
    for ch in range(len(chunks)):
        for swap in swaps(ch):
            swap.wait_send()


def finish_kernel(*refs):
    count = (len(refs) - 1) // 2
    sem = refs[-1]
    memory, new_memory = refs[0], refs[count]
    copies = []
    for b in range(memory.shape[0] // BLOCK):
        part = pl.ds(b * BLOCK, BLOCK)
        copies.append(
            pltpu.make_async_copy(memory.at[part], new_memory.at[part], sem.at[count - 1 + b])
        )
    for i, (src, dst) in enumerate(zip(refs[1:count], refs[count + 1 : 2 * count])):
        copies.append(pltpu.make_async_copy(src, dst, sem.at[i]))
    for copy in copies:
        copy.start()
    for copy in copies:
        copy.wait()


def shards(
    n, tokens, norm_gain, w_query, w_key, w_value, w_outgate, w_input, w_forget, forget_bias,
    head_gain, w_out, memory, normalizer, stabilizer, prev_keys, prev_values, prev_input,
    prev_forget, accepted,
):
    seqs, span, width = tokens.shape
    depth, heads, keys = w_query.shape
    values = w_value.shape[2]
    rows = seqs * span
    hk, hv = heads * keys, heads * values
    all_heads = w_input.shape[1]
    sds = jax.ShapeDtypeStruct
    vm = pl.BlockSpec(memory_space=pltpu.VMEM)
    hbm = pl.BlockSpec(memory_space=pl.ANY)
    flip = lambda w: w.transpose(1, 2, 0).reshape(-1, depth)

    parts = sum(CHUNKS)
    unit = rows // parts
    lanes = -(-unit * max(CHUNKS) // 128) * 128
    count = len(CHUNKS)
    blocks = seqs // BLOCK
    hp = -(-heads // 8) * 8
    channels = 2 * hk + 2 * hv + 2 * all_heads
    dma = lambda *shape: pltpu.SemaphoreType.DMA(shape)
    outs = [
        sds(tokens.shape, BF16), sds((seqs, span, heads, keys), BF16),
        sds((seqs, span, heads, values), BF16), sds(memory.shape, F32),
        sds(normalizer.shape, F32), sds((heads, seqs), F32),
        sds((span, heads, seqs), F32), sds((span, heads, seqs), F32),
    ]
    y, k, v, mem, new_n, ns, ni, nf = pl.pallas_call(
        functools.partial(fused_kernel, n, keys, head_gain.shape[1]),
        out_shape=outs,
        in_specs=[vm] * 11 + [hbm] * 8,
        out_specs=[vm] * 8,
        scratch_shapes=[
            pltpu.VMEM((2 * n, rows, width), BF16),
            pltpu.VMEM((channels, depth), BF16),
            pltpu.VMEM((count, channels, lanes), F32),
            pltpu.VMEM((count, lanes, 128), F32),
            pltpu.VMEM((hv, rows), BF16),
            pltpu.VMEM((heads, rows, 2 * keys), BF16),
            pltpu.VMEM((heads, seqs, keys), F32),
            pltpu.VMEM((heads, seqs // 4, values, 4 * keys), BF16),
            pltpu.VMEM((heads, seqs, keys), BF16),
            pltpu.VMEM((2, hp, count * lanes), F32),
            pltpu.VMEM((hp, count * lanes), F32),
            pltpu.VMEM((rows, hk), BF16),
            pltpu.VMEM((rows, hv), BF16),
            pltpu.VMEM((rows, heads, keys), F32),
            pltpu.VMEM((rows, heads, values), F32),
            pltpu.VMEM((count, hv, lanes), BF16),
            pltpu.VMEM((count, heads, lanes), F32),
            pltpu.VMEM((count, hv, lanes), BF16),
            pltpu.VMEM((count, heads, lanes), F32),
            pltpu.VMEM((rows, 2 * hv), BF16),
            pltpu.VMEM((n, 2 * hv, width), BF16),
        ]
        + [pltpu.VMEM((n, rows, width), BF16)] * 4
        + [
            pltpu.VMEM((2, lanes, width), F32), pltpu.VMEM((rows, width), F32),
            dma(6), dma(blocks), dma(n), dma(n), dma(n),
            dma(3, 2 * n, PIECES), dma(2 * n, PIECES), dma(count, n), dma(count, 2 * n),
            dma(count, 2 * n), dma(count, 2), dma(count, 2),
        ]
        + [dma(n, rows // PIECE)] * 4,
        compiler_params=pltpu.CompilerParams(
            collective_id=0, has_side_effects=True, vmem_limit_bytes=FUSED_LIMIT
        ),
        name="fused",
    )(
        *[
            pltpu.with_memory_space_constraint(a, pltpu.HBM)
            for a in (
                tokens, norm_gain.reshape(1, depth), forget_bias.reshape(1, all_heads),
                prev_keys, prev_values, prev_input.transpose(1, 2, 0),
                prev_forget.transpose(1, 2, 0), accepted.reshape(1, seqs), stabilizer.T,
                normalizer, head_gain,
                flip(w_query), flip(w_key), flip(w_value), flip(w_outgate),
                w_input.T, w_forget.T, memory, w_out.reshape(hv, -1),
            )
        ]
    )

    new_memory, y, k, v, new_n, ns, ni, nf = pl.pallas_call(
        finish_kernel,
        out_shape=[outs[3], *outs[:3], *outs[4:]],
        in_specs=[vm] * 8,
        out_specs=[hbm] * 8,
        scratch_shapes=[dma(7 + blocks)],
        compiler_params=pltpu.CompilerParams(vmem_limit_bytes=FINISH_LIMIT),
        name="finish",
    )(mem, y, k, v, new_n, ns, ni, nf)

    return y, new_memory, new_n, ns.T, k, v, ni.transpose(2, 0, 1), nf.transpose(2, 0, 1)


def solution(mesh):
    return jax.shard_map(
        functools.partial(shards, mesh.shape["kv"]),
        mesh=mesh,
        in_specs=(
            P(("grp", "dp"), None, ("kv", "tp")),
            P(),
            P(None, "kv", None),
            P(None, "kv", None),
            P(None, "kv", "tp"),
            P(None, "kv", "tp"),
            P(),
            P(),
            P(),
            P(),
            P("kv", "tp", None),
            P(("grp", "dp"), "kv", "tp", None),
            P(("grp", "dp"), "kv", None),
            P(("grp", "dp"), "kv"),
            P(("grp", "dp"), None, "kv", None),
            P(("grp", "dp"), None, "kv", "tp"),
            P(("grp", "dp"), None, "kv"),
            P(("grp", "dp"), None, "kv"),
            P(("grp", "dp")),
        ),
        out_specs=(
            P(("grp", "dp"), None, ("kv", "tp")),
            P(("grp", "dp"), "kv", "tp", None),
            P(("grp", "dp"), "kv", None),
            P(("grp", "dp"), "kv"),
            P(("grp", "dp"), None, "kv", None),
            P(("grp", "dp"), None, "kv", "tp"),
            P(("grp", "dp"), None, "kv"),
            P(("grp", "dp"), None, "kv"),
        ),
        check_vma=False,
    )
```
